32 devices in a mesh: sp: 16 (over z, y, x), tp: 2 (over core).
Axes of the slice: x: 2, y: 2, z: 4, core: 2. Of those that a mesh axis runs over, the one named last changes fastest.
Arguments:
- residual: bfloat16 [4096, 2048], P(('sp', 'tp')), may hold values from -6 to 6
- projected: bfloat16 [4096, 2048], P('sp', 'tp'), may hold values from -6 to 6
- group_weight: bfloat16 [4, 512, 512], P('tp'), may hold values from -0.25 to 0.25
- channel_scale: float32 [2048], P('tp'), may hold values from 0.1 to 1.9
- out_weight: bfloat16 [2048, 2048], replicated, may hold values from -0.125 to 0.125
- post_mix_gain: float32 [2048], replicated, may hold values from 0.1 to 1.9
- pre_ffn_gain: float32 [2048], replicated, may hold values from 0.1 to 1.9
- post_ffn_gain: float32 [2048], replicated, may hold values from 0.1 to 1.9
- route_ids: int32 [4096, 2], P(('sp', 'tp')), may hold values from 0 to 7, all different within a row; in each aligned block of 128 rows (0 to 127, 128 to 255, ...) at most 64 rows name the same one
- route_weight: float32 [4096, 2], P(('sp', 'tp')), may hold values from 0.1 to 1
- expert_gate: bfloat16 [16, 2048, 1792], P('sp', None, 'tp'), may hold values from -0.125 to 0.125
- expert_up: bfloat16 [16, 2048, 1792], P('sp', None, 'tp'), may hold values from -0.125 to 0.125
- expert_down: bfloat16 [16, 1792, 2048], P('sp', 'tp'), may hold values from -0.09375 to 0.09375
Outputs:
- layer_out: bfloat16 [4096, 2048], P(('sp', 'tp'))
The draws below stay inside these ranges and needn't reach their ends.
Inputs may be any that keep to these rules, and one draw needn't show every extreme that they name: `route_ids`: each row names 2 different experts. In every aligned block of 128 rows (the rows of one device) no expert is named more than 64 times, a bound that some blocks reach.
All inputs are finite; a program needn't handle non-finite values.
Results may differ from the reference program's by a relative error of at most 0.014.
Values may be sent and summed in bfloat16 or wider, within the bound.
A program may use at most 192 MiB of HBM per device.

```python
import math
import jax
import jax.numpy as jnp
import numpy as np
from jax import lax

D = 2048
GROUPS = 4
GROUP_W = 512
FF = 3584
TOP = 2
TOKENS = 4096
ROWS_DEV = 128
EXPERTS = 8
HALVES = 16
CAP = 64
N_SP = 16
N_TP = 2


def steps_of(key, extent, split, low, top_value):
    loudness, own = 1.0, jax.random.fold_in(key, 6)
    for dim, parts in split:
        heights = jnp.exp(jax.random.uniform(jax.random.fold_in(own, dim), (parts,), jnp.float32, low / len(split), top_value / len(split)))
        loudness = loudness * jnp.repeat(heights, extent[dim] // parts).reshape([-1 if axis == dim else 1 for axis in range(len(extent))])
    return loudness


def assign_block(key, own, number, rows, number_of, top, limit, slope):
    sequence = jax.random.permutation(key, number_of)
    heavy_load, usual = load_shares(number_of, rows * top, limit, slope, True), load_shares(number_of, rows * top, limit, slope, False)
    places = jnp.arange(number_of)

    def named(sizes, rotation):
        used = int((sizes > 0).sum())
        fixed = max(1, used // 4)
        passed = fixed + (places - fixed + rotation * (used - fixed)) % max(1, number_of - fixed)
        return jnp.zeros((number_of,), jnp.int32).at[sequence[jnp.where(places < fixed, places, passed)]].set(jnp.asarray(sizes, jnp.int32))

    sizes = jnp.where(number % 4 == 0, named(heavy_load, number // 4), named(usual, number - number // 4 - 1))
    mixed = jax.random.permutation(jax.random.fold_in(own, 3), number_of)
    giver, receiver = mixed[0:number_of // 2 * 2:2], mixed[1:number_of // 2 * 2:2]
    margin = jnp.minimum(sizes[giver] - 1, limit - sizes[receiver]) // 2
    margin = jnp.where((giver == sequence[0]) | (receiver == sequence[0]) | (sizes[receiver] == 0), 0, jnp.maximum(margin, 0))
    passed = jax.random.randint(jax.random.fold_in(own, 4), (number_of // 2,), 0, 1 << 20) % (margin + 1)
    sizes = sizes.at[giver].add(-passed).at[receiver].add(passed)
    members = jnp.searchsorted(jnp.cumsum(sizes), jnp.arange(rows * top), side="right").astype(jnp.int32)
    listing = members.reshape(top, rows).T
    listing = listing[jax.random.permutation(jax.random.fold_in(own, 1), rows)]
    rotation = jax.random.randint(jax.random.fold_in(own, 2), (rows, 1), 0, top)
    return jnp.take_along_axis(listing, (jnp.arange(top)[None, :] + rotation) % top, axis=1)


def load_shares(number_of, total, most, slope, full):
    weights = [(1 << 20) // math.isqrt(grade ** slope) + 1 for grade in range(1, number_of + 1)]
    largest = most if full else min(most, max(-(-total // number_of), total * weights[0] // sum(weights)))
    least = 1 if total - largest >= number_of - 1 else 0
    given, spare = [largest] + [least] * (number_of - 1), total - largest - least * (number_of - 1)
    while spare > 0:
        movable = [i for i in range(1, number_of) if given[i] < largest] or [i for i in range(1, number_of) if given[i] < most]
        pool, remaining = sum([weights[i] for i in movable]), spare
        for i in movable:
            extra = min(most - given[i], max(1, remaining * weights[i] // pool), spare)
            given[i] = given[i] + extra
            spare = spare - extra
    return np.array(given)


def scatter_about(rng, dims, width, limit, shards=(), kind=jnp.bfloat16):
    result = jax.random.normal(rng, dims, jnp.float32) * width
    if len(shards) > 0:
        result = steps_of(rng, dims, shards, -0.22, 0.18) * result
    return jnp.clip(result, min=-limit, max=limit).astype(kind)


def setup_inputs(seed: int = 0) -> dict:
    keys = jax.random.split(jax.random.key(seed), 14)
    residual = scatter_about(keys[0], (TOKENS, D), 1.0, 6.0, ((0, 32),))
    projected = scatter_about(keys[1], (TOKENS, D), 1.0, 6.0, ((0, 16), (1, 2)))
    group_weight = scatter_about(keys[2], (GROUPS, GROUP_W, GROUP_W), GROUP_W ** -0.5, 0.25, ((0, 2),))
    channel_scale = jnp.clip(1.0 + 0.18 * jax.random.normal(keys[3], (D,), jnp.float32), 0.1, 1.9)
    out_weight = scatter_about(keys[4], (D, D), D ** -0.5, 0.125)
    post_mix_gain = jnp.clip(1.0 + 0.18 * jax.random.normal(keys[5], (D,), jnp.float32), 0.1, 1.9)
    pre_ffn_gain = jnp.clip(1.0 + 0.18 * jax.random.normal(keys[6], (D,), jnp.float32), 0.1, 1.9)
    post_ffn_gain = jnp.clip(1.0 + 0.18 * jax.random.normal(keys[7], (D,), jnp.float32), 0.1, 1.9)
    route_ids_keys = jax.random.split(jax.random.fold_in(keys[8], 1), TOKENS // ROWS_DEV)
    route_ids_turns = jax.random.permutation(jax.random.fold_in(keys[8], 3), TOKENS // ROWS_DEV)
    route_ids = jax.vmap(lambda own, number: assign_block(jax.random.fold_in(keys[8], 2), own, number, ROWS_DEV, EXPERTS, TOP, CAP, 2))(route_ids_keys, route_ids_turns).reshape((TOKENS, TOP))
    route_weight = jnp.clip(0.1 + 0.9 * jax.random.uniform(keys[9], (TOKENS, TOP), jnp.float32) ** steps_of(keys[9], (TOKENS, TOP), ((0, 32),), -0.2, 0.2), 0.1, 1.0)
    expert_gate = scatter_about(keys[10], (HALVES, D, FF // 2), D ** -0.5, 0.125, ((0, 16), (2, 2)))
    expert_up = scatter_about(keys[11], (HALVES, D, FF // 2), D ** -0.5, 0.125, ((0, 16), (2, 2)))
    expert_down = scatter_about(keys[12], (HALVES, FF // 2, D), FF ** -0.5, 0.09375, ((0, 16), (1, 2)))
    return dict(residual=residual, projected=projected, group_weight=group_weight, channel_scale=channel_scale, out_weight=out_weight, post_mix_gain=post_mix_gain, pre_ffn_gain=pre_ffn_gain, post_ffn_gain=post_ffn_gain, route_ids=route_ids, route_weight=route_weight, expert_gate=expert_gate, expert_up=expert_up, expert_down=expert_down)


EPS = 1e-06

def rms_scale(values, gain):
    values = values.astype(jnp.float32)
    inverse = lax.rsqrt(lax.optimization_barrier(jnp.mean(values * values, axis=-1, keepdims=True)) + EPS)
    return values * inverse * gain.astype(jnp.float32)

def window_sums(extended, lookback, count):
    levels = []
    current = extended
    window_span = 1
    for level_id in range(GROUPS):
        current = current[window_span:] + current[:-window_span]
        window_span = window_span * 2
        first = lookback - window_span + 1
        levels.append(lax.slice_in_dim(current, first, first + count, axis=0))
    return levels

def expert_output(token_rows, expert_id, expert_gate, expert_up, expert_down):
    quarter = FF // (2 * N_TP)
    total = jnp.zeros((token_rows.shape[0], D), jnp.float32)
    for half_id in range(2):
        entry = (2 * expert_id + half_id).astype(jnp.int32)
        gate_half = lax.dynamic_index_in_dim(expert_gate, entry, 0, keepdims=False)
        up_half = lax.dynamic_index_in_dim(expert_up, entry, 0, keepdims=False)
        down_half = lax.dynamic_index_in_dim(expert_down, entry, 0, keepdims=False)
        partial_value = jnp.zeros((token_rows.shape[0], D), jnp.float32)
        for part_id in range(N_TP):
            low = part_id * quarter
            gate_value = jnp.dot(token_rows, gate_half[:, low:low + quarter], preferred_element_type=jnp.float32)
            up_value = jnp.dot(token_rows, up_half[:, low:low + quarter], preferred_element_type=jnp.float32)
            active = (jax.nn.silu(gate_value) * up_value).astype(jnp.bfloat16)
            term = jnp.dot(active, down_half[low:low + quarter], preferred_element_type=jnp.float32).astype(jnp.bfloat16)
            partial_value = partial_value + term.astype(jnp.float32)
        total = total + partial_value.astype(jnp.bfloat16).astype(jnp.float32)
    rounded = lax.optimization_barrier(total.astype(jnp.bfloat16))
    return rounded.astype(jnp.float32)

def reference(residual, projected, group_weight, channel_scale, out_weight, post_mix_gain, pre_ffn_gain, post_ffn_gain, route_ids, route_weight, expert_gate, expert_up, expert_down):
    lookback = 2 ** GROUPS
    count = projected.shape[0]
    extended = jnp.concatenate([jnp.zeros((lookback, D), jnp.float32), projected.astype(jnp.float32)], 0)
    levels = window_sums(extended, lookback, count)
    position = (jnp.arange(count, dtype=jnp.int32) + 1).astype(jnp.float32)[:, None]
    pieces = []
    for group_id in range(GROUPS):
        low = group_id * GROUP_W
        window_span = jnp.float32(2.0 ** (group_id + 1))
        own_part = projected[:, low:low + GROUP_W].astype(jnp.float32)
        pieces.append(levels[group_id][:, low:low + GROUP_W] / jnp.minimum(position, window_span) - own_part)
    pooled = jnp.concatenate(pieces, 1).astype(jnp.bfloat16)
    grouped = jnp.einsum('tgc,gce->tge', pooled.reshape(count, GROUPS, GROUP_W).astype(jnp.float32), group_weight.astype(jnp.float32))
    scaled = (grouped.reshape(count, D) * channel_scale.astype(jnp.float32)).astype(jnp.bfloat16)
    mixed = jnp.dot(scaled, out_weight, preferred_element_type=jnp.float32).astype(jnp.bfloat16)
    middle = (residual.astype(jnp.float32) + rms_scale(mixed, post_mix_gain)).astype(jnp.bfloat16)
    normed = rms_scale(middle, pre_ffn_gain).astype(jnp.bfloat16)
    flat_ids = route_ids.reshape(-1).astype(jnp.int32)
    flat_weight = route_weight.reshape(-1).astype(jnp.float32)
    order = jnp.argsort(flat_ids, stable=True).astype(jnp.int32)
    onehot = (flat_ids[:, None] == jnp.arange(EXPERTS, dtype=jnp.int32)[None, :]).astype(jnp.int32)
    counts = lax.optimization_barrier(jnp.sum(onehot, 0)).astype(jnp.int32)
    starts = (jnp.cumsum(counts) - counts).astype(jnp.int32)
    most = CAP * N_SP * N_TP
    order_padded = jnp.concatenate([order, jnp.zeros((most,), jnp.int32)])

    def add_expert(total, expert_id):
        picks = lax.dynamic_slice_in_dim(order_padded, starts[expert_id].astype(jnp.int32), most)
        live = jnp.arange(most, dtype=jnp.int32) < counts[expert_id]
        token_ids = (picks // TOP).astype(jnp.int32)
        outputs = expert_output(normed[token_ids], expert_id, expert_gate, expert_up, expert_down)
        factor = jnp.where(live, flat_weight[picks], jnp.float32(0.0))
        return (total.at[token_ids].add(outputs * factor[:, None]), None)
    ffn_sum, _ = lax.scan(add_expert, jnp.zeros((count, D), jnp.float32), jnp.arange(EXPERTS, dtype=jnp.int32))
    return (middle.astype(jnp.float32) + rms_scale(ffn_sum, post_ffn_gain)).astype(jnp.bfloat16)
```

```python
import functools

import jax
import jax.numpy as jnp
from jax import lax
from jax.experimental import pallas as pl
from jax.experimental.pallas import tpu as pltpu
from jax.sharding import PartitionSpec as P

GROUPS = 4
TOP = 2


EPS = 1e-06
MESH = pl.DeviceIdType.MESH
TILE = 256
WIDE = 512
GROUP_ROWS = 256


def rms_scale(values, gain):
    inverse = lax.rsqrt(jnp.mean(values * values, axis=-1, keepdims=True) + EPS)
    return values * inverse * gain


def flipped(index, mask, count):
    result = 0
    bit = 1
    while bit < count:
        digit = (index // bit) % 2
        result = result + (1 - digit if mask & bit else digit) * bit
        bit = bit * 2
    return result


def layer_kernel(
    experts,
    cap,
    residual,
    projected,
    group_weight,
    channel_scale,
    out_hbm,
    post_mix_gain,
    pre_ffn_gain,
    post_ffn_gain,
    route_ids,
    route_weight,
    gate_hbm,
    up_hbm,
    down_hbm,
    result,
    gate_all,
    up_all,
    down_all,
    rows,
    active,
    partial,
    mirrored,
    table,
    back,
    out_all,
    halo,
    scaled,
    received,
    mixed,
    middle,
    local_sem,
    weight_send,
    weight_recv,
    out_send,
    out_recv,
    twin_send,
    twin_recv,
    swap_send,
    swap_recv,
    back_send,
    back_recv,
    front_send,
    front_recv,
):
    place = lax.axis_index("sp")
    core = lax.axis_index("tp")
    expert, side = place // 2, place % 2
    twin = (place + 1 - 2 * side, core)
    partner = (place, 1 - core)
    peers = [None] + [(2 * flipped(expert, r, experts) + side, core) for r in range(1, experts)]
    quarter = gate_hbm.shape[2]
    hidden = 2 * quarter
    width = residual.shape[1]
    half_rows = GROUP_ROWS // 2
    per_group = half_rows // cap
    places = lax.axis_size("sp")
    tokens = projected.shape[0]
    share = tokens // 2
    cut = projected.shape[1]
    lookback = halo.shape[0]
    groups = experts // per_group

    def spot(r, mirror):
        return (r // per_group) * GROUP_ROWS + mirror * half_rows + (r % per_group) * cap

    def send(source, target, device, first, second):
        copy = pltpu.make_async_remote_copy(
            src_ref=source,
            dst_ref=target,
            send_sem=first,
            recv_sem=second,
            device_id=device,
            device_id_type=MESH,
        )
        copy.start()
        return copy

    weights = [
        (gate_hbm.at[0], gate_all.at[:, pl.ds(0, quarter)], gate_all.at[:, pl.ds(quarter, quarter)]),
        (up_hbm.at[0], up_all.at[:, pl.ds(0, quarter)], up_all.at[:, pl.ds(quarter, quarter)]),
        (down_hbm.at[0], down_all.at[pl.ds(0, quarter)], down_all.at[pl.ds(quarter, quarter)]),
    ]
    out_load = pltpu.make_async_copy(out_hbm, out_all, local_sem.at[3])
    out_load.start()
    loads = []
    for i, (source, own, _) in enumerate(weights):
        load = pltpu.make_async_copy(source, own, local_sem.at[i])
        load.start()
        loads.append(load)

    barrier = pltpu.get_barrier_semaphore()
    ring = [((place + 1) % places, core), ((place + places - 1) % places, core)]
    for device in peers[1:] + [twin, partner] + ring:
        pl.semaphore_signal(barrier, inc=1, device_id=device, device_id_type=MESH)
    pl.semaphore_wait(barrier, experts + 3)

    edge = pltpu.make_async_remote_copy(
        src_ref=projected.at[pl.ds(tokens - lookback, lookback)],
        dst_ref=halo,
        send_sem=front_send.at[0],
        recv_sem=front_recv.at[0],
        device_id=ring[0],
        device_id_type=MESH,
    )

    @pl.when(place < places - 1)
    def _():
        edge.start()

    columns = lax.broadcasted_iota(jnp.int32, (share, experts * cap), 1)
    owner = (columns // cap) ^ expert
    named = [owner == route_ids[:, k : k + 1] for k in range(TOP)]
    member = functools.reduce(jnp.logical_or, named).astype(jnp.float32)
    earlier = (
        lax.broadcasted_iota(jnp.int32, (share, share), 1)
        < lax.broadcasted_iota(jnp.int32, (share, share), 0)
    ).astype(jnp.bfloat16)
    rank = jnp.dot(earlier, member.astype(jnp.bfloat16), preferred_element_type=jnp.float32)
    chosen = jnp.where(rank == (columns % cap).astype(jnp.float32), member, 0.0)
    spread = chosen.T.astype(jnp.bfloat16)
    picks = [jnp.where(hit, chosen, 0.0).astype(jnp.bfloat16) for hit in named]

    @pl.when(place > 0)
    def _():
        edge.wait_recv()

    @pl.when(place == 0)
    def _():
        halo[...] = jnp.zeros_like(halo)

    position = (
        place * tokens + lax.broadcasted_iota(jnp.int32, (tokens, 1), 0) + 1
    ).astype(jnp.float32)
    groups_here = group_weight.shape[0]
    group_width = cut // groups_here
    for local_group in range(groups_here):
        low = local_group * group_width
        own_part = projected[:, low : low + group_width].astype(jnp.float32)
        current = jnp.concatenate(
            [halo[:, low : low + group_width].astype(jnp.float32), own_part], 0
        )
        group_id = core * groups_here + local_group
        summed = own_part
        window_span = jnp.float32(1.0)
        for level_id in range(GROUPS):
            current = current + pltpu.roll(current, 2**level_id, 0)
            hit = group_id == level_id
            summed = jnp.where(hit, current[lookback:], summed)
            window_span = jnp.where(hit, jnp.float32(2.0 ** (level_id + 1)), window_span)
        pooled = (summed / jnp.minimum(position, window_span) - own_part).astype(jnp.bfloat16)
        grouped = jnp.dot(pooled, group_weight[local_group], preferred_element_type=jnp.float32)
        scaled[:, low : low + group_width] = (
            grouped * channel_scale[:, low : low + group_width]
        ).astype(jnp.bfloat16)
    there = pl.ds(pl.multiple_of((1 - core) * share, share), share)
    here = pl.ds(pl.multiple_of(core * share, share), share)
    exchange = send(scaled.at[there], received, partner, front_send.at[1], front_recv.at[1])
    out_load.wait()

    def mix(block, first_row, fresh):
        def step(t, carry):
            at = pl.ds(pl.multiple_of(t * WIDE, WIDE), WIDE)
            value = jnp.dot(
                block, out_all[pl.ds(first_row, cut), at], preferred_element_type=jnp.float32
            )
            mixed[:, at] = value if fresh else mixed[:, at] + value
            return carry

        lax.fori_loop(0, width // WIDE, step, 0)

    mix(scaled[here], pl.multiple_of(core * cut, cut), True)
    exchange.wait_recv()
    gathers = [
        send(source, theirs, partner, weight_send.at[i], weight_recv.at[i])
        for i, (source, _, theirs) in enumerate(weights)
    ]
    mix(received[...], pl.multiple_of((1 - core) * cut, cut), False)
    rounded = mixed[...].astype(jnp.bfloat16).astype(jnp.float32)
    kept = residual[...].astype(jnp.float32) + rms_scale(rounded, post_mix_gain[...])
    middle[...] = kept.astype(jnp.bfloat16)
    normed = rms_scale(middle[...].astype(jnp.float32), pre_ffn_gain[...]).astype(jnp.bfloat16)
    for low in range(0, width, WIDE):
        block = jnp.dot(spread, normed[:, low : low + WIDE], preferred_element_type=jnp.float32)
        table[:, :, low : low + WIDE] = block.astype(jnp.bfloat16).reshape(experts, cap, WIDE)
    rows[pl.ds(spot(0, 0), cap)] = table[0]

    outs = [None] + [
        send(
            table.at[r],
            rows.at[pl.ds(spot(r, 0), cap)],
            peers[r],
            out_send.at[r],
            out_recv.at[r],
        )
        for r in range(1, experts)
    ]
    twins = [None] * experts
    twins[0] = send(
        table.at[0], rows.at[pl.ds(spot(0, 1), cap)], twin, twin_send.at[0], twin_recv.at[0]
    )
    swaps = [None] * experts
    backs = [None] * experts

    def forward(g):
        for r in range(g * per_group, (g + 1) * per_group):
            if r > 0:
                outs[r].wait_recv()
                twins[r] = send(
                    rows.at[pl.ds(spot(r, 0), cap)],
                    rows.at[pl.ds(spot(r, 1), cap)],
                    twin,
                    twin_send.at[r],
                    twin_recv.at[r],
                )

    def compute(g):
        base = g * GROUP_ROWS
        for r in range(g * per_group, (g + 1) * per_group):
            twins[r].wait_recv()
        if g == 0:
            for i in range(2):
                loads[i].wait()
                gathers[i].wait_recv()

        def enter(t, carry):
            at = pl.ds(pl.multiple_of(t * TILE, TILE), TILE)
            here = rows[pl.ds(base, GROUP_ROWS), :]
            gate = jnp.dot(here, gate_all[:, at], preferred_element_type=jnp.float32)
            up = jnp.dot(here, up_all[:, at], preferred_element_type=jnp.float32)
            active[:, at] = (jax.nn.silu(gate) * up).astype(jnp.bfloat16)
            return carry

        lax.fori_loop(0, hidden // TILE, enter, 0)
        if g == 0:
            loads[2].wait()
            gathers[2].wait_recv()

        def leave(t, carry):
            at = pl.ds(pl.multiple_of(t * TILE, TILE), TILE)
            value = jnp.dot(active[...], down_all[:, at], preferred_element_type=jnp.float32)
            partial[pl.ds(base, GROUP_ROWS), at] = value.astype(jnp.bfloat16)
            return carry

        lax.fori_loop(0, width // TILE, leave, 0)

    def swap(g):
        for r in range(g * per_group, (g + 1) * per_group):
            swaps[r] = send(
                partial.at[pl.ds(spot(r, 1), cap)],
                mirrored.at[r],
                twin,
                swap_send.at[r],
                swap_recv.at[r],
            )

    def finish(g):
        for r in range(g * per_group, (g + 1) * per_group):
            piece = pl.ds(spot(r, 0), cap)
            swaps[r].wait_recv()
            total = partial[piece].astype(jnp.float32) + mirrored[r].astype(jnp.float32)
            partial[piece] = total.astype(jnp.bfloat16)
            if r > 0:
                backs[r] = send(
                    partial.at[piece], back.at[r], peers[r], back_send.at[r], back_recv.at[r]
                )
            else:
                back[0] = partial[piece]

    forward(0)
    forward(1)
    compute(0)
    forward(2)
    swap(0)
    compute(2)
    swap(2)
    forward(3)
    compute(1)
    swap(1)
    finish(0)
    finish(2)
    compute(3)
    swap(3)
    finish(1)
    finish(3)
    for r in range(1, experts):
        backs[r].wait_recv()
    flat = back[...].reshape(experts * cap, width)
    for low in range(0, width, WIDE):
        total = jnp.zeros((share, WIDE), jnp.float32)
        for k in range(TOP):
            picked = jnp.dot(
                picks[k], flat[:, low : low + WIDE], preferred_element_type=jnp.float32
            )
            total = total + picked * route_weight[:, k : k + 1]
        mixed[:, low : low + WIDE] = total
    result[...] = (
        middle[...].astype(jnp.float32) + rms_scale(mixed[...], post_ffn_gain[...])
    ).astype(jnp.bfloat16)
    for r in range(1, experts):
        backs[r].wait_send()
        outs[r].wait_send()
    for copy in twins + swaps + gathers + [exchange]:
        copy.wait_send()

    @pl.when(place < places - 1)
    def _():
        edge.wait_send()


def line_kernel(
    experts,
    cap,
    residual,
    projected,
    group_weight,
    channel_scale,
    out_hbm,
    post_mix_gain,
    pre_ffn_gain,
    post_ffn_gain,
    route_ids,
    route_weight,
    gate_hbm,
    up_hbm,
    down_hbm,
    result,
    gate_all,
    up_all,
    down_all,
    out_all,
    raw,
    rows,
    across,
    active,
    partial,
    mirrored,
    back,
    halo,
    scaled,
    received,
    mixed,
    middle,
    ids,
    picks,
    weigh,
    local_sem,
    weight_send,
    weight_recv,
    front_send,
    front_recv,
    ids_send,
    ids_recv,
    raw_send,
    raw_recv,
    y_send,
    y_recv,
    x_send,
    x_recv,
    swap_send,
    swap_recv,
    back_send,
    back_recv,
):
    place = lax.axis_index("sp")
    core = lax.axis_index("tp")
    places = lax.axis_size("sp")
    planes = places // 4
    last = planes - 1
    z, y, x = place // 4, (place // 2) % 2, place % 2
    half = z // (planes // 2)
    inward = 1 - 2 * half
    own = (z + half) % 2
    partner = (place, 1 - core)
    quarter = gate_hbm.shape[2]
    hidden = 2 * quarter
    share, width = residual.shape
    tokens, cut = projected.shape
    lookback = halo.shape[0]
    block_rows = 4 * cap
    piece = share // 2

    def spot(s, other_y, other_x):
        at_z = s + half * (last - 2 * s)
        at_y = 1 - y if other_y else y
        at_x = 1 - x if other_x else x
        return (at_z * 4 + at_y * 2 + at_x, core)

    def remote(source, target, device, first, second):
        return pltpu.make_async_remote_copy(
            src_ref=source,
            dst_ref=target,
            send_sem=first,
            recv_sem=second,
            device_id=device,
            device_id_type=MESH,
        )

    weights = [
        (gate_hbm.at[0], gate_all.at[:, pl.ds(0, quarter)], gate_all.at[:, pl.ds(quarter, quarter)]),
        (up_hbm.at[0], up_all.at[:, pl.ds(0, quarter)], up_all.at[:, pl.ds(quarter, quarter)]),
        (down_hbm.at[0], down_all.at[pl.ds(0, quarter)], down_all.at[pl.ds(quarter, quarter)]),
    ]
    out_load = pltpu.make_async_copy(out_hbm, out_all, local_sem.at[3])
    out_load.start()
    loads = []
    for i, (source, mine, _) in enumerate(weights):
        load = pltpu.make_async_copy(source, mine, local_sem.at[i])
        load.start()
        loads.append(load)

    barrier = pltpu.get_barrier_semaphore()
    for step in range(1, places):
        device = ((place + step) % places, core)
        pl.semaphore_signal(barrier, inc=1, device_id=device, device_id_type=MESH)
    pl.semaphore_signal(barrier, inc=1, device_id=partner, device_id_type=MESH)
    pl.semaphore_wait(barrier, places)

    edge = remote(
        projected.at[pl.ds(tokens - lookback, lookback)],
        halo,
        ((place + 1) % places, core),
        front_send.at[0],
        front_recv.at[0],
    )

    @pl.when(place < places - 1)
    def _():
        edge.start()

    ids[own] = jnp.concatenate(
        [route_ids[...], jnp.zeros((ids.shape[1] - TOP, share), jnp.int32)], 0
    )

    def id_copies(role):
        if role == 0:
            targets = [(1, False, 0), (2, False, 3), (3, False, 3)]
            targets += [(0, True, 4), (1, True, 4), (2, True, 5), (3, True, 5)]
        else:
            targets = [(0, False, 1), (2, False, 2), (3, False, 2)]
        return [
            remote(ids.at[role], ids.at[j], spot(s, False, turn), ids_send.at[i], ids_recv.at[j])
            for i, (s, turn, j) in enumerate(targets)
        ]

    def expect(target, semaphore):
        return remote(target, target, partner, local_sem.at[0], semaphore)

    for role in range(2):

        @pl.when(own == role)
        def _(role=role):
            for copy in id_copies(role):
                copy.start()

    for role in range(2):

        @pl.when(own == role)
        def _(role=role):
            for j in range(6):
                if j != role:
                    expect(ids.at[j], ids_recv.at[j]).wait_recv()

    sub = lax.broadcasted_iota(jnp.int32, (8, share), 0)
    here_expert = 2 * z + jnp.where(sub == 0, y, 1 - y)
    at = sub // 2
    turn = sub % 2
    home_expert = 2 * (at + half * (last - 2 * at)) + (y + turn - 2 * y * turn)
    members = []
    for j in range(6):
        first, second = ids[j, 0:1, :], ids[j, 1:2, :]
        named = jnp.logical_or(first == here_expert, second == here_expert)
        members.append(jnp.where(jnp.logical_and(named, sub < 2), 1.0, 0.0))
    first, second = route_ids[0:1, :] == home_expert, route_ids[1:2, :] == home_expert
    members.append(jnp.where(jnp.logical_or(first, second), 1.0, 0.0))
    factor = jnp.where(first, route_weight[0:1, :], 0.0) + jnp.where(
        second, route_weight[1:2, :], 0.0
    )
    member = jnp.concatenate(members, 0)
    earlier = jnp.where(
        lax.broadcasted_iota(jnp.int32, (share, share), 0)
        < lax.broadcasted_iota(jnp.int32, (share, share), 1),
        1.0,
        0.0,
    ).astype(jnp.bfloat16)
    rank = jnp.dot(member.astype(jnp.bfloat16), earlier, preferred_element_type=jnp.float32)
    slot = lax.broadcasted_iota(jnp.int32, (cap, share), 0).astype(jnp.float32)
    for j in range(6):
        pair = [
            jnp.where(rank[8 * j + i : 8 * j + i + 1] == slot, member[8 * j + i : 8 * j + i + 1], 0.0)
            for i in range(2)
        ]
        picks[j] = jnp.concatenate(pair, 0).astype(jnp.bfloat16)
    for s in range(4):
        pair = [
            jnp.where(rank[48 + i : 49 + i] == slot, factor[i : i + 1], 0.0)
            for i in (2 * s, 2 * s + 1)
        ]
        full = jnp.concatenate(pair, 0).T
        high = full.astype(jnp.bfloat16)
        weigh[s, 0] = high
        weigh[s, 1] = (full - high.astype(jnp.float32)).astype(jnp.bfloat16)

    @pl.when(place > 0)
    def _():
        edge.wait_recv()

    @pl.when(place == 0)
    def _():
        halo[...] = jnp.zeros_like(halo)

    position = (
        place * tokens + lax.broadcasted_iota(jnp.int32, (tokens, 1), 0) + 1
    ).astype(jnp.float32)
    groups_here = group_weight.shape[0]
    group_width = cut // groups_here
    for local_group in range(groups_here):
        low = local_group * group_width
        own_part = projected[:, low : low + group_width].astype(jnp.float32)
        current = jnp.concatenate(
            [halo[:, low : low + group_width].astype(jnp.float32), own_part], 0
        )
        group_id = core * groups_here + local_group
        summed = own_part
        window_span = jnp.float32(1.0)
        for level_id in range(GROUPS):
            current = current + pltpu.roll(current, 2**level_id, 0)
            hit = group_id == level_id
            summed = jnp.where(hit, current[lookback:], summed)
            window_span = jnp.where(hit, jnp.float32(2.0 ** (level_id + 1)), window_span)
        pooled = (summed / jnp.minimum(position, window_span) - own_part).astype(jnp.bfloat16)
        grouped = jnp.dot(pooled, group_weight[local_group], preferred_element_type=jnp.float32)
        scaled[:, low : low + group_width] = (
            grouped * channel_scale[:, low : low + group_width]
        ).astype(jnp.bfloat16)
    there = pl.ds(pl.multiple_of((1 - core) * share, share), share)
    here = pl.ds(pl.multiple_of(core * share, share), share)
    exchange = remote(scaled.at[there], received, partner, front_send.at[1], front_recv.at[1])
    exchange.start()
    out_load.wait()

    def mix(block, first_row, fresh):
        def step(t, carry):
            at = pl.ds(pl.multiple_of(t * WIDE, WIDE), WIDE)
            value = jnp.dot(
                block, out_all[pl.ds(first_row, cut), at], preferred_element_type=jnp.float32
            )
            mixed[:, at] = value if fresh else mixed[:, at] + value
            return carry

        lax.fori_loop(0, width // WIDE, step, 0)

    mix(scaled[here], pl.multiple_of(core * cut, cut), True)
    exchange.wait_recv()
    gathers = [
        remote(source, theirs, partner, weight_send.at[i], weight_recv.at[i])
        for i, (source, _, theirs) in enumerate(weights)
    ]
    for copy in gathers:
        copy.start()
    mix(received[...], pl.multiple_of((1 - core) * cut, cut), False)
    rounded = mixed[...].astype(jnp.bfloat16).astype(jnp.float32)
    kept = residual[...].astype(jnp.float32) + rms_scale(rounded, post_mix_gain[...])
    middle[...] = kept.astype(jnp.bfloat16)
    raw[own] = rms_scale(middle[...].astype(jnp.float32), pre_ffn_gain[...]).astype(jnp.bfloat16)

    def program(role):
        sent = list(id_copies(role))
        state = {"loaded": False}

        def launch(copy):
            copy.start()
            sent.append(copy)

        def raw_out(number, source, target, device, part):
            span = pl.ds(part * piece, piece)
            launch(
                remote(
                    raw.at[source, span],
                    raw.at[target, span],
                    device,
                    raw_send.at[number, part],
                    raw_recv.at[target, part],
                )
            )

        def raw_in(j, part):
            span = pl.ds(part * piece, piece)
            expect(raw.at[j, span], raw_recv.at[j, part]).wait_recv()

        def row_of(j):
            return j * block_rows if j < 4 else (j - 4) * 3 * block_rows + 2 * cap

        def select(j):
            low = row_of(j)

            def step(t, carry):
                at = pl.ds(pl.multiple_of(t * WIDE, WIDE), WIDE)
                value = jnp.dot(picks[j], raw[j, :, at], preferred_element_type=jnp.float32)
                value = value.astype(jnp.bfloat16)
                rows[pl.ds(low, cap), at] = value[:cap]
                across[j, :, at] = value[cap:]
                return carry

            lax.fori_loop(0, width // WIDE, step, 0)
            launch(
                remote(
                    across.at[j],
                    rows.at[pl.ds(low + cap, cap)],
                    spot(role, True, False),
                    y_send.at[j],
                    y_recv.at[j],
                )
            )

        def y_in(j):
            expect(rows.at[pl.ds(row_of(j) + cap, cap)], y_recv.at[j]).wait_recv()

        def x_out(s, side):
            low = s * block_rows + side * cap
            number = 2 * (s - 1) + side
            launch(
                remote(
                    rows.at[pl.ds(low, cap)],
                    rows.at[pl.ds(low + 2 * cap, cap)],
                    spot(role, False, True),
                    x_send.at[number],
                    x_recv.at[number],
                )
            )

        def x_in(s, side):
            low = s * block_rows + (2 + side) * cap
            expect(rows.at[pl.ds(low, cap)], x_recv.at[2 * (s - 1) + side]).wait_recv()

        def compute(s):
            base = s * block_rows
            if not state["loaded"]:
                for i in range(2):
                    loads[i].wait()
                    gathers[i].wait_recv()

            def enter(t, carry):
                at = pl.ds(pl.multiple_of(t * TILE, TILE), TILE)
                block = rows[pl.ds(base, block_rows), :]
                gate = jnp.dot(block, gate_all[:, at], preferred_element_type=jnp.float32)
                up = jnp.dot(block, up_all[:, at], preferred_element_type=jnp.float32)
                active[:, at] = (jax.nn.silu(gate) * up).astype(jnp.bfloat16)
                return carry

            lax.fori_loop(0, hidden // TILE, enter, 0)
            if not state["loaded"]:
                loads[2].wait()
                gathers[2].wait_recv()
            state["loaded"] = True

            def leave(t, carry):
                at = pl.ds(pl.multiple_of(t * TILE, TILE), TILE)
                value = jnp.dot(active[...], down_all[:, at], preferred_element_type=jnp.float32)
                partial[pl.ds(base, block_rows), at] = value.astype(jnp.bfloat16)
                return carry

            lax.fori_loop(0, width // TILE, leave, 0)

        def swap(s, side):
            span = pl.ds(side * cap, cap)
            launch(
                remote(
                    partial.at[pl.ds(s * block_rows + (2 + side) * cap, cap)],
                    mirrored.at[s, span],
                    spot(role, False, True),
                    swap_send.at[s, side],
                    swap_recv.at[s, side],
                )
            )

        def finish(s, side):
            arrived = mirrored.at[s, pl.ds(side * cap, cap)]
            expect(arrived, swap_recv.at[s, side]).wait_recv()
            seen = role if s < 2 else last - role
            span = pl.ds(s * block_rows + side * cap, cap)
            total = partial[span].astype(jnp.float32) + arrived[...].astype(jnp.float32)
            if s == role and side == 0:
                back[2 * s] = total.astype(jnp.bfloat16)
                return
            partial[span] = total.astype(jnp.bfloat16)
            launch(
                remote(
                    partial.at[span],
                    back.at[2 * seen + side],
                    spot(s, side == 1, False),
                    back_send.at[2 * s + side],
                    back_recv.at[2 * seen + side],
                )
            )

        def gather(s, fresh):
            for side in range(2):
                if s != role or side == 1:
                    expect(back.at[2 * s + side], back_recv.at[2 * s + side]).wait_recv()
            for low in range(0, width, WIDE):
                block = back[2 * s : 2 * s + 2, :, low : low + WIDE].reshape(2 * cap, WIDE)
                value = jnp.dot(weigh[s, 0], block, preferred_element_type=jnp.float32)
                value = value + jnp.dot(weigh[s, 1], block, preferred_element_type=jnp.float32)
                held = mixed[:, low : low + WIDE]
                mixed[:, low : low + WIDE] = value if fresh else held + value

        near = spot(1 - role, False, False)
        twin = spot(role, False, True)
        if role == 0:
            for part in range(2):
                raw_out(0, 0, 0, near, part)
                raw_out(1, 0, 4, twin, part)
            select(0)
            raw_in(4, 0)
            raw_out(2, 4, 4, near, 0)
            raw_in(1, 0)
            raw_in(1, 1)
            select(1)
            x_out(1, 0)
            raw_in(4, 1)
            raw_out(2, 4, 4, near, 1)
            select(4)
            y_in(1)
            x_out(1, 1)
            raw_in(2, 0)
            raw_in(2, 1)
            select(2)
            x_out(2, 0)
            y_in(0)
            y_in(4)
            compute(0)
            y_in(2)
            x_out(2, 1)
            x_in(1, 0)
            x_in(1, 1)
            compute(1)
            swap(0, 1)
            raw_in(3, 0)
            raw_in(3, 1)
            select(3)
            x_in(2, 0)
            x_in(2, 1)
            compute(2)
            swap(2, 0)
            swap(2, 1)
            swap(1, 0)
            finish(0, 1)
            raw_in(5, 0)
            raw_in(5, 1)
            select(5)
            finish(2, 0)
            finish(2, 1)
            y_in(3)
            y_in(5)
            compute(3)
            swap(3, 0)
            swap(3, 1)
            swap(1, 1)
            swap(0, 0)
            finish(1, 0)
            finish(3, 0)
            finish(3, 1)
            gather(1, True)
            finish(1, 1)
            gather(2, False)
            finish(0, 0)
            gather(0, False)
            gather(3, False)
        else:
            far = spot(2, False, False)
            for part in range(2):
                raw_out(0, 1, 1, near, part)
                raw_out(1, 1, 2, far, part)
            select(1)
            x_out(1, 0)
            y_in(1)
            x_out(1, 1)
            for part in range(2):
                raw_in(0, part)
                raw_out(2, 0, 3, far, part)
                raw_in(2, part)
                raw_out(3, 2, 2, near, part)
            select(2)
            x_out(2, 0)
            select(0)
            y_in(2)
            x_out(2, 1)
            raw_in(3, 0)
            raw_out(4, 3, 3, near, 0)
            raw_in(4, 0)
            raw_out(5, 4, 5, far, 0)
            x_in(1, 0)
            x_in(1, 1)
            compute(1)
            swap(1, 1)
            raw_in(3, 1)
            raw_out(4, 3, 3, near, 1)
            raw_in(4, 1)
            raw_out(5, 4, 5, far, 1)
            select(3)
            select(4)
            x_in(2, 0)
            x_in(2, 1)
            compute(2)
            swap(2, 0)
            swap(2, 1)
            for part in range(2):
                raw_in(5, part)
                raw_out(6, 5, 5, near, part)
            select(5)
            y_in(0)
            y_in(4)
            compute(0)
            swap(0, 0)
            swap(0, 1)
            finish(2, 0)
            finish(2, 1)
            y_in(3)
            y_in(5)
            compute(3)
            swap(3, 0)
            swap(3, 1)
            swap(1, 0)
            finish(1, 1)
            finish(0, 0)
            finish(0, 1)
            finish(3, 0)
            finish(3, 1)
            gather(2, True)
            finish(1, 0)
            gather(3, False)
            gather(1, False)
            gather(0, False)
        result[...] = (
            middle[...].astype(jnp.float32) + rms_scale(mixed[...], post_ffn_gain[...])
        ).astype(jnp.bfloat16)
        for copy in sent + gathers + [exchange]:
            copy.wait_send()

    for role in range(2):

        @pl.when(own == role)
        def _(role=role):
            program(role)

    @pl.when(place < places - 1)
    def _():
        edge.wait_send()


def body(
    residual,
    projected,
    group_weight,
    channel_scale,
    out_weight,
    post_mix_gain,
    pre_ffn_gain,
    post_ffn_gain,
    route_ids,
    route_weight,
    expert_gate,
    expert_up,
    expert_down,
):
    share, width = residual.shape
    tokens, cut = projected.shape
    experts = lax.axis_size("sp") // 2
    cap = 2 * TOP * share // experts
    quarter = expert_gate.shape[2]
    kinds = jnp.bfloat16
    dma = pltpu.SemaphoreType.DMA
    vmem = pl.BlockSpec(memory_space=pltpu.VMEM)
    hbm = pl.BlockSpec(memory_space=pltpu.HBM)
    if 4 * 4 == lax.axis_size("sp"):
        sizes = [
            (width, 2 * quarter),
            (width, 2 * quarter),
            (2 * quarter, width),
            out_weight.shape,
            (6, share, width),
            (2 * experts * cap, width),
            (6, cap, width),
            (4 * cap, 2 * quarter),
            (2 * experts * cap, width),
            (4, 2 * cap, width),
            (experts, cap, width),
            (2**GROUPS, cut),
            (tokens, cut),
            (share, cut),
        ]
        return pl.pallas_call(
            functools.partial(line_kernel, experts, cap),
            out_shape=jax.ShapeDtypeStruct((share, width), kinds),
            in_specs=[vmem] * 4 + [hbm] + [vmem] * 5 + [hbm] * 3,
            out_specs=vmem,
            scratch_shapes=[pltpu.VMEM(size, kinds) for size in sizes]
            + [
                pltpu.VMEM((share, width), jnp.float32),
                pltpu.VMEM((share, width), kinds),
                pltpu.VMEM((6, 8, share), jnp.int32),
                pltpu.VMEM((6, 2 * cap, share), kinds),
                pltpu.VMEM((4, 2, share, 2 * cap), kinds),
                dma((4,)),
                dma((3,)),
                dma((3,)),
                dma((2,)),
                dma((2,)),
                dma((7,)),
                dma((6,)),
                dma((7, 2)),
                dma((6, 2)),
                dma((6,)),
                dma((6,)),
                dma((4,)),
                dma((4,)),
                dma((4, 2)),
                dma((4, 2)),
                dma((8,)),
                dma((8,)),
            ],
            compiler_params=pltpu.CompilerParams(
                collective_id=0, has_side_effects=True, vmem_limit_bytes=62 * 1024 * 1024
            ),
        )(
            residual,
            projected,
            group_weight,
            channel_scale.reshape(1, cut),
            out_weight,
            post_mix_gain.reshape(1, width),
            pre_ffn_gain.reshape(1, width),
            post_ffn_gain.reshape(1, width),
            route_ids.T,
            route_weight.T,
            expert_gate,
            expert_up,
            expert_down,
        )
    return pl.pallas_call(
        functools.partial(layer_kernel, experts, cap),
        out_shape=jax.ShapeDtypeStruct((share, width), kinds),
        in_specs=[vmem] * 4 + [hbm] + [vmem] * 5 + [hbm] * 3,
        out_specs=vmem,
        scratch_shapes=[
            pltpu.VMEM((width, 2 * quarter), kinds),
            pltpu.VMEM((width, 2 * quarter), kinds),
            pltpu.VMEM((2 * quarter, width), kinds),
            pltpu.VMEM((2 * experts * cap, width), kinds),
            pltpu.VMEM((GROUP_ROWS, 2 * quarter), kinds),
            pltpu.VMEM((2 * experts * cap, width), kinds),
            pltpu.VMEM((experts, cap, width), kinds),
            pltpu.VMEM((experts, cap, width), kinds),
            pltpu.VMEM((experts, cap, width), kinds),
            pltpu.VMEM(out_weight.shape, kinds),
            pltpu.VMEM((2**GROUPS, cut), kinds),
            pltpu.VMEM((tokens, cut), kinds),
            pltpu.VMEM((share, cut), kinds),
            pltpu.VMEM((share, width), jnp.float32),
            pltpu.VMEM((share, width), kinds),
            dma((4,)),
            dma((3,)),
            dma((3,)),
        ]
        + [dma((experts,))] * 8
        + [dma((2,))] * 2,
        compiler_params=pltpu.CompilerParams(
            collective_id=0, has_side_effects=True, vmem_limit_bytes=62 * 1024 * 1024
        ),
    )(
        residual,
        projected,
        group_weight,
        channel_scale.reshape(1, cut),
        out_weight,
        post_mix_gain.reshape(1, width),
        pre_ffn_gain.reshape(1, width),
        post_ffn_gain.reshape(1, width),
        route_ids,
        route_weight,
        expert_gate,
        expert_up,
        expert_down,
    )


def solution(mesh):
    in_specs = (
        P(("sp", "tp"), None),
        P("sp", "tp"),
        P("tp", None, None),
        P("tp"),
        P(),
        P(),
        P(),
        P(),
        P(("sp", "tp"), None),
        P(("sp", "tp"), None),
        P("sp", None, "tp"),
        P("sp", None, "tp"),
        P("sp", "tp", None),
    )
    out_specs = P(("sp", "tp"), None)
    return jax.shard_map(body, mesh=mesh, in_specs=in_specs, out_specs=out_specs, check_vma=False)
```

```python
import functools

import jax
import jax.numpy as jnp
from jax import lax
from jax.experimental import pallas as pl
from jax.experimental.pallas import tpu as pltpu
from jax.sharding import PartitionSpec as P

GROUPS = 4
TOP = 2


EPS = 1e-06
MESH = pl.DeviceIdType.MESH
TILE = 256
WIDE = 512
GROUP_ROWS = 256


def rms_scale(values, gain):
    inverse = lax.rsqrt(jnp.mean(values * values, axis=-1, keepdims=True) + EPS)
    return values * inverse * gain


def flipped(index, mask, count):
    result = 0
    bit = 1
    while bit < count:
        digit = (index // bit) % 2
        result = result + (1 - digit if mask & bit else digit) * bit
        bit = bit * 2
    return result


def layer_kernel(
    experts,
    cap,
    residual,
    projected,
    group_weight,
    channel_scale,
    out_hbm,
    post_mix_gain,
    pre_ffn_gain,
    post_ffn_gain,
    route_ids,
    route_weight,
    gate_hbm,
    up_hbm,
    down_hbm,
    result,
    gate_all,
    up_all,
    down_all,
    rows,
    active,
    partial,
    mirrored,
    table,
    back,
    out_all,
    halo,
    scaled,
    received,
    mixed,
    middle,
    local_sem,
    weight_send,
    weight_recv,
    out_send,
    out_recv,
    twin_send,
    twin_recv,
    swap_send,
    swap_recv,
    back_send,
    back_recv,
    front_send,
    front_recv,
):
    place = lax.axis_index("sp")
    core = lax.axis_index("tp")
    expert, side = place // 2, place % 2
    twin = (place + 1 - 2 * side, core)
    partner = (place, 1 - core)
    peers = [None] + [(2 * flipped(expert, r, experts) + side, core) for r in range(1, experts)]
    quarter = gate_hbm.shape[2]
    hidden = 2 * quarter
    width = residual.shape[1]
    half_rows = GROUP_ROWS // 2
    per_group = half_rows // cap
    places = lax.axis_size("sp")
    tokens = projected.shape[0]
    share = tokens // 2
    cut = projected.shape[1]
    lookback = halo.shape[0]
    groups = experts // per_group

    def spot(r, mirror):
        return (r // per_group) * GROUP_ROWS + mirror * half_rows + (r % per_group) * cap

    def send(source, target, device, first, second):
        copy = pltpu.make_async_remote_copy(
            src_ref=source,
            dst_ref=target,
            send_sem=first,
            recv_sem=second,
            device_id=device,
            device_id_type=MESH,
        )
        copy.start()
        return copy

    weights = [
        (gate_hbm.at[0], gate_all.at[:, pl.ds(0, quarter)], gate_all.at[:, pl.ds(quarter, quarter)]),
        (up_hbm.at[0], up_all.at[:, pl.ds(0, quarter)], up_all.at[:, pl.ds(quarter, quarter)]),
        (down_hbm.at[0], down_all.at[pl.ds(0, quarter)], down_all.at[pl.ds(quarter, quarter)]),
    ]
    out_load = pltpu.make_async_copy(out_hbm, out_all, local_sem.at[3])
    out_load.start()
    loads = []
    for i, (source, own, _) in enumerate(weights):
        load = pltpu.make_async_copy(source, own, local_sem.at[i])
        load.start()
        loads.append(load)

    barrier = pltpu.get_barrier_semaphore()
    ring = [((place + 1) % places, core), ((place + places - 1) % places, core)]
    for device in peers[1:] + [twin, partner] + ring:
        pl.semaphore_signal(barrier, inc=1, device_id=device, device_id_type=MESH)
    pl.semaphore_wait(barrier, experts + 3)

    edge = pltpu.make_async_remote_copy(
        src_ref=projected.at[pl.ds(tokens - lookback, lookback)],
        dst_ref=halo,
        send_sem=front_send.at[0],
        recv_sem=front_recv.at[0],
        device_id=ring[0],
        device_id_type=MESH,
    )

    @pl.when(place < places - 1)
    def _():
        edge.start()

    columns = lax.broadcasted_iota(jnp.int32, (share, experts * cap), 1)
    owner = (columns // cap) ^ expert
    named = [owner == route_ids[:, k : k + 1] for k in range(TOP)]
    member = functools.reduce(jnp.logical_or, named).astype(jnp.float32)
    earlier = (
        lax.broadcasted_iota(jnp.int32, (share, share), 1)
        < lax.broadcasted_iota(jnp.int32, (share, share), 0)
    ).astype(jnp.bfloat16)
    rank = jnp.dot(earlier, member.astype(jnp.bfloat16), preferred_element_type=jnp.float32)
    chosen = jnp.where(rank == (columns % cap).astype(jnp.float32), member, 0.0)
    spread = chosen.T.astype(jnp.bfloat16)
    picks = [jnp.where(hit, chosen, 0.0).astype(jnp.bfloat16) for hit in named]

    @pl.when(place > 0)
    def _():
        edge.wait_recv()

    @pl.when(place == 0)
    def _():
        halo[...] = jnp.zeros_like(halo)

    position = (
        place * tokens + lax.broadcasted_iota(jnp.int32, (tokens, 1), 0) + 1
    ).astype(jnp.float32)
    groups_here = group_weight.shape[0]
    group_width = cut // groups_here
    for local_group in range(groups_here):
        low = local_group * group_width
        own_part = projected[:, low : low + group_width].astype(jnp.float32)
        current = jnp.concatenate(
            [halo[:, low : low + group_width].astype(jnp.float32), own_part], 0
        )
        group_id = core * groups_here + local_group
        summed = own_part
        window_span = jnp.float32(1.0)
        for level_id in range(GROUPS):
            current = current + pltpu.roll(current, 2**level_id, 0)
            hit = group_id == level_id
            summed = jnp.where(hit, current[lookback:], summed)
            window_span = jnp.where(hit, jnp.float32(2.0 ** (level_id + 1)), window_span)
        pooled = (summed / jnp.minimum(position, window_span) - own_part).astype(jnp.bfloat16)
        grouped = jnp.dot(pooled, group_weight[local_group], preferred_element_type=jnp.float32)
        scaled[:, low : low + group_width] = (
            grouped * channel_scale[:, low : low + group_width]
        ).astype(jnp.bfloat16)
    there = pl.ds(pl.multiple_of((1 - core) * share, share), share)
    here = pl.ds(pl.multiple_of(core * share, share), share)
    exchange = send(scaled.at[there], received, partner, front_send.at[1], front_recv.at[1])
    out_load.wait()

    def mix(block, first_row, fresh):
        def step(t, carry):
            at = pl.ds(pl.multiple_of(t * WIDE, WIDE), WIDE)
            value = jnp.dot(
                block, out_all[pl.ds(first_row, cut), at], preferred_element_type=jnp.float32
            )
            mixed[:, at] = value if fresh else mixed[:, at] + value
            return carry

        lax.fori_loop(0, width // WIDE, step, 0)

    mix(scaled[here], pl.multiple_of(core * cut, cut), True)
    exchange.wait_recv()
    gathers = [
        send(source, theirs, partner, weight_send.at[i], weight_recv.at[i])
        for i, (source, _, theirs) in enumerate(weights)
    ]
    mix(received[...], pl.multiple_of((1 - core) * cut, cut), False)
    rounded = mixed[...].astype(jnp.bfloat16).astype(jnp.float32)
    kept = residual[...].astype(jnp.float32) + rms_scale(rounded, post_mix_gain[...])
    middle[...] = kept.astype(jnp.bfloat16)
    normed = rms_scale(middle[...].astype(jnp.float32), pre_ffn_gain[...]).astype(jnp.bfloat16)
    for low in range(0, width, WIDE):
        block = jnp.dot(spread, normed[:, low : low + WIDE], preferred_element_type=jnp.float32)
        table[:, :, low : low + WIDE] = block.astype(jnp.bfloat16).reshape(experts, cap, WIDE)
    rows[pl.ds(spot(0, 0), cap)] = table[0]

    outs = [None] + [
        send(
            table.at[r],
            rows.at[pl.ds(spot(r, 0), cap)],
            peers[r],
            out_send.at[r],
            out_recv.at[r],
        )
        for r in range(1, experts)
    ]
    twins = [None] * experts
    twins[0] = send(
        table.at[0], rows.at[pl.ds(spot(0, 1), cap)], twin, twin_send.at[0], twin_recv.at[0]
    )
    swaps = [None] * experts
    backs = [None] * experts

    def forward(g):
        for r in range(g * per_group, (g + 1) * per_group):
            if r > 0:
                outs[r].wait_recv()
                twins[r] = send(
                    rows.at[pl.ds(spot(r, 0), cap)],
                    rows.at[pl.ds(spot(r, 1), cap)],
                    twin,
                    twin_send.at[r],
                    twin_recv.at[r],
                )

    def compute(g):
        base = g * GROUP_ROWS
        for r in range(g * per_group, (g + 1) * per_group):
            twins[r].wait_recv()
        if g == 0:
            for i in range(2):
                loads[i].wait()
                gathers[i].wait_recv()

        def enter(t, carry):
            at = pl.ds(pl.multiple_of(t * TILE, TILE), TILE)
            here = rows[pl.ds(base, GROUP_ROWS), :]
            gate = jnp.dot(here, gate_all[:, at], preferred_element_type=jnp.float32)
            up = jnp.dot(here, up_all[:, at], preferred_element_type=jnp.float32)
            active[:, at] = (jax.nn.silu(gate) * up).astype(jnp.bfloat16)
            return carry

        lax.fori_loop(0, hidden // TILE, enter, 0)
        if g == 0:
            loads[2].wait()
            gathers[2].wait_recv()

        def leave(t, carry):
            at = pl.ds(pl.multiple_of(t * TILE, TILE), TILE)
            value = jnp.dot(active[...], down_all[:, at], preferred_element_type=jnp.float32)
            partial[pl.ds(base, GROUP_ROWS), at] = value.astype(jnp.bfloat16)
            return carry

        lax.fori_loop(0, width // TILE, leave, 0)

    def swap(g):
        for r in range(g * per_group, (g + 1) * per_group):
            swaps[r] = send(
                partial.at[pl.ds(spot(r, 1), cap)],
                mirrored.at[r],
                twin,
                swap_send.at[r],
                swap_recv.at[r],
            )

    def finish(g):
        for r in range(g * per_group, (g + 1) * per_group):
            piece = pl.ds(spot(r, 0), cap)
            swaps[r].wait_recv()
            total = partial[piece].astype(jnp.float32) + mirrored[r].astype(jnp.float32)
            partial[piece] = total.astype(jnp.bfloat16)
            if r > 0:
                backs[r] = send(
                    partial.at[piece], back.at[r], peers[r], back_send.at[r], back_recv.at[r]
                )
            else:
                back[0] = partial[piece]

    forward(0)
    forward(1)
    compute(0)
    forward(2)
    swap(0)
    compute(2)
    swap(2)
    forward(3)
    compute(1)
    swap(1)
    finish(0)
    finish(2)
    compute(3)
    swap(3)
    finish(1)
    finish(3)
    for r in range(1, experts):
        backs[r].wait_recv()
    flat = back[...].reshape(experts * cap, width)
    for low in range(0, width, WIDE):
        total = jnp.zeros((share, WIDE), jnp.float32)
        for k in range(TOP):
            picked = jnp.dot(
                picks[k], flat[:, low : low + WIDE], preferred_element_type=jnp.float32
            )
            total = total + picked * route_weight[:, k : k + 1]
        mixed[:, low : low + WIDE] = total
    result[...] = (
        middle[...].astype(jnp.float32) + rms_scale(mixed[...], post_ffn_gain[...])
    ).astype(jnp.bfloat16)
    for r in range(1, experts):
        backs[r].wait_send()
        outs[r].wait_send()
    for copy in twins + swaps + gathers + [exchange]:
        copy.wait_send()

    @pl.when(place < places - 1)
    def _():
        edge.wait_send()


def line_kernel(
    experts,
    cap,
    residual,
    projected,
    group_weight,
    channel_scale,
    out_hbm,
    post_mix_gain,
    pre_ffn_gain,
    post_ffn_gain,
    route_ids,
    route_weight,
    gate_hbm,
    up_hbm,
    down_hbm,
    result,
    gate_all,
    up_all,
    down_all,
    out_all,
    raw,
    rows,
    across,
    active,
    partial,
    mirrored,
    back,
    halo,
    scaled,
    received,
    mixed,
    middle,
    ids,
    picks,
    weigh,
    local_sem,
    weight_send,
    weight_recv,
    front_send,
    front_recv,
    ids_send,
    ids_recv,
    raw_send,
    raw_recv,
    y_send,
    y_recv,
    x_send,
    x_recv,
    swap_send,
    swap_recv,
    back_send,
    back_recv,
):
    place = lax.axis_index("sp")
    core = lax.axis_index("tp")
    places = lax.axis_size("sp")
    planes = places // 4
    last = planes - 1
    z, y, x = place // 4, (place // 2) % 2, place % 2
    half = z // (planes // 2)
    inward = 1 - 2 * half
    own = (z + half) % 2
    partner = (place, 1 - core)
    quarter = gate_hbm.shape[2]
    hidden = 2 * quarter
    share, width = residual.shape
    tokens, cut = projected.shape
    lookback = halo.shape[0]
    block_rows = 4 * cap
    piece = share // 2
    up_tile = hidden // 2

    def spot(s, other_y, other_x):
        at_z = s + half * (last - 2 * s)
        at_y = 1 - y if other_y else y
        at_x = 1 - x if other_x else x
        return (at_z * 4 + at_y * 2 + at_x, core)

    def remote(source, target, device, first, second):
        return pltpu.make_async_remote_copy(
            src_ref=source,
            dst_ref=target,
            send_sem=first,
            recv_sem=second,
            device_id=device,
            device_id_type=MESH,
        )

    weights = [
        (gate_hbm.at[0], gate_all.at[:, pl.ds(0, quarter)], gate_all.at[:, pl.ds(quarter, quarter)]),
        (up_hbm.at[0], up_all.at[:, pl.ds(0, quarter)], up_all.at[:, pl.ds(quarter, quarter)]),
        (down_hbm.at[0], down_all.at[pl.ds(0, quarter)], down_all.at[pl.ds(quarter, quarter)]),
    ]
    out_load = pltpu.make_async_copy(out_hbm, out_all, local_sem.at[3])
    out_load.start()
    loads = []
    for i, (source, mine, _) in enumerate(weights):
        load = pltpu.make_async_copy(source, mine, local_sem.at[i])
        load.start()
        loads.append(load)

    barrier = pltpu.get_barrier_semaphore()
    for step in range(1, places):
        device = ((place + step) % places, core)
        pl.semaphore_signal(barrier, inc=1, device_id=device, device_id_type=MESH)
    pl.semaphore_signal(barrier, inc=1, device_id=partner, device_id_type=MESH)
    pl.semaphore_wait(barrier, places)

    edge = remote(
        projected.at[pl.ds(tokens - lookback, lookback)],
        halo,
        ((place + 1) % places, core),
        front_send.at[0],
        front_recv.at[0],
    )

    @pl.when(place < places - 1)
    def _():
        edge.start()

    ids[own] = jnp.concatenate(
        [route_ids[...], jnp.zeros((ids.shape[1] - TOP, share), jnp.int32)], 0
    )

    def id_copies(role):
        if role == 0:
            targets = [(1, False, 0), (2, False, 3), (3, False, 3)]
            targets += [(0, True, 4), (1, True, 4), (2, True, 5), (3, True, 5)]
        else:
            targets = [(0, False, 1), (2, False, 2), (3, False, 2)]
        return [
            remote(ids.at[role], ids.at[j], spot(s, False, turn), ids_send.at[i], ids_recv.at[j])
            for i, (s, turn, j) in enumerate(targets)
        ]

    def expect(target, semaphore):
        return remote(target, target, partner, local_sem.at[0], semaphore)

    for role in range(2):

        @pl.when(own == role)
        def _(role=role):
            for copy in id_copies(role):
                copy.start()

    @pl.when(place > 0)
    def _():
        edge.wait_recv()

    @pl.when(place == 0)
    def _():
        halo[...] = jnp.zeros_like(halo)

    position = (
        place * tokens + lax.broadcasted_iota(jnp.int32, (tokens, 1), 0) + 1
    ).astype(jnp.float32)
    groups_here = group_weight.shape[0]
    group_width = cut // groups_here
    for local_group in range(groups_here):
        low = local_group * group_width
        own_part = projected[:, low : low + group_width].astype(jnp.float32)
        current = jnp.concatenate(
            [halo[:, low : low + group_width].astype(jnp.float32), own_part], 0
        )
        group_id = core * groups_here + local_group
        summed = own_part
        window_span = jnp.float32(1.0)
        for level_id in range(GROUPS):
            current = current + pltpu.roll(current, 2**level_id, 0)
            hit = group_id == level_id
            summed = jnp.where(hit, current[lookback:], summed)
            window_span = jnp.where(hit, jnp.float32(2.0 ** (level_id + 1)), window_span)
        pooled = (summed / jnp.minimum(position, window_span) - own_part).astype(jnp.bfloat16)
        grouped = jnp.dot(pooled, group_weight[local_group], preferred_element_type=jnp.float32)
        scaled[:, low : low + group_width] = (
            grouped * channel_scale[:, low : low + group_width]
        ).astype(jnp.bfloat16)
    there = pl.ds(pl.multiple_of((1 - core) * share, share), share)
    here = pl.ds(pl.multiple_of(core * share, share), share)
    exchange = remote(scaled.at[there], received, partner, front_send.at[1], front_recv.at[1])
    exchange.start()
    out_load.wait()

    def mix(block, first_row, fresh):
        def step(t, carry):
            at = pl.ds(pl.multiple_of(t * WIDE, WIDE), WIDE)
            value = jnp.dot(
                block, out_all[pl.ds(first_row, cut), at], preferred_element_type=jnp.float32
            )
            mixed[:, at] = value if fresh else mixed[:, at] + value
            return carry

        lax.fori_loop(0, width // WIDE, step, 0)

    mix(scaled[here], pl.multiple_of(core * cut, cut), True)
    exchange.wait_recv()
    gathers = [
        remote(source, theirs, partner, weight_send.at[i], weight_recv.at[i])
        for i, (source, _, theirs) in enumerate(weights)
    ]
    for copy in gathers:
        copy.start()
    mix(received[...], pl.multiple_of((1 - core) * cut, cut), False)
    rounded = mixed[...].astype(jnp.bfloat16).astype(jnp.float32)
    kept = residual[...].astype(jnp.float32) + rms_scale(rounded, post_mix_gain[...])
    middle[...] = kept.astype(jnp.bfloat16)
    raw[own] = rms_scale(middle[...].astype(jnp.float32), pre_ffn_gain[...]).astype(jnp.bfloat16)

    def raw_copy(number, source, target, device, part):
        span = pl.ds(part * piece, piece)
        return remote(
            raw.at[source, span],
            raw.at[target, span],
            device,
            raw_send.at[number, part],
            raw_recv.at[target, part],
        )

    def first_copies(role):
        near, twin = spot(1 - role, False, False), spot(role, False, True)
        copies = []
        for part in range(2):
            if role == 0:
                copies.append(raw_copy(0, 0, 0, near, part))
                copies.append(raw_copy(1, 0, 4, twin, part))
            else:
                copies.append(raw_copy(0, 1, 1, near, part))
                copies.append(raw_copy(1, 1, 2, spot(2, False, False), part))
        return copies

    for role in range(2):

        @pl.when(own == role)
        def _(role=role):
            for copy in first_copies(role):
                copy.start()

    for role in range(2):

        @pl.when(own == role)
        def _(role=role):
            for j in range(6):
                if j != role:
                    expect(ids.at[j], ids_recv.at[j]).wait_recv()

    sub = lax.broadcasted_iota(jnp.int32, (8, share), 0)
    here_expert = 2 * z + jnp.where(sub == 0, y, 1 - y)
    at = sub // 2
    turn = sub % 2
    home_expert = 2 * (at + half * (last - 2 * at)) + (y + turn - 2 * y * turn)
    members = []
    for j in range(6):
        first, second = ids[j, 0:1, :], ids[j, 1:2, :]
        named = jnp.logical_or(first == here_expert, second == here_expert)
        members.append(jnp.where(jnp.logical_and(named, sub < 2), 1.0, 0.0))
    first, second = route_ids[0:1, :] == home_expert, route_ids[1:2, :] == home_expert
    members.append(jnp.where(jnp.logical_or(first, second), 1.0, 0.0))
    factor = jnp.where(first, route_weight[0:1, :], 0.0) + jnp.where(
        second, route_weight[1:2, :], 0.0
    )
    member = jnp.concatenate(members, 0)
    earlier = jnp.where(
        lax.broadcasted_iota(jnp.int32, (share, share), 0)
        < lax.broadcasted_iota(jnp.int32, (share, share), 1),
        1.0,
        0.0,
    ).astype(jnp.bfloat16)
    rank = jnp.dot(member.astype(jnp.bfloat16), earlier, preferred_element_type=jnp.float32)
    slot = lax.broadcasted_iota(jnp.int32, (cap, share), 0).astype(jnp.float32)
    for j in range(6):
        pair = [
            jnp.where(rank[8 * j + i : 8 * j + i + 1] == slot, member[8 * j + i : 8 * j + i + 1], 0.0)
            for i in range(2)
        ]
        picks[j] = jnp.concatenate(pair, 0).astype(jnp.bfloat16)
    for s in range(4):
        pair = [
            jnp.where(rank[48 + i : 49 + i] == slot, factor[i : i + 1], 0.0)
            for i in (2 * s, 2 * s + 1)
        ]
        full = jnp.concatenate(pair, 0).T
        high = full.astype(jnp.bfloat16)
        weigh[s, 0] = high
        weigh[s, 1] = (full - high.astype(jnp.float32)).astype(jnp.bfloat16)

    def program(role):
        sent = id_copies(role) + first_copies(role)
        state = {"entered": False, "left": False, "summed": False}

        def launch(copy):
            copy.start()
            sent.append(copy)

        def raw_out(*hop):
            launch(raw_copy(*hop))

        def raw_in(j, part):
            span = pl.ds(part * piece, piece)
            expect(raw.at[j, span], raw_recv.at[j, part]).wait_recv()

        def row_of(j):
            return j * block_rows if j < 4 else (j - 4) * 3 * block_rows + 2 * cap

        def select(j):
            low = row_of(j)

            def step(t, carry):
                at = pl.ds(pl.multiple_of(t * WIDE, WIDE), WIDE)
                value = jnp.dot(picks[j], raw[j, :, at], preferred_element_type=jnp.float32)
                value = value.astype(jnp.bfloat16)
                rows[pl.ds(low, cap), at] = value[:cap]
                across[j, :, at] = value[cap:]
                return carry

            lax.fori_loop(0, width // WIDE, step, 0)
            launch(
                remote(
                    across.at[j],
                    rows.at[pl.ds(low + cap, cap)],
                    spot(role, True, False),
                    y_send.at[j],
                    y_recv.at[j],
                )
            )

        def y_in(j):
            expect(rows.at[pl.ds(row_of(j) + cap, cap)], y_recv.at[j]).wait_recv()

        def x_out(s, side):
            low = s * block_rows + side * cap
            number = 2 * (s - 1) + side
            launch(
                remote(
                    rows.at[pl.ds(low, cap)],
                    rows.at[pl.ds(low + 2 * cap, cap)],
                    spot(role, False, True),
                    x_send.at[number],
                    x_recv.at[number],
                )
            )

        def x_in(s, side):
            low = s * block_rows + (2 + side) * cap
            expect(rows.at[pl.ds(low, cap)], x_recv.at[2 * (s - 1) + side]).wait_recv()

        def enter(s):
            base = s * block_rows
            if not state["entered"]:
                for i in range(2):
                    loads[i].wait()
                    gathers[i].wait_recv()
            state["entered"] = True

            def step(t, carry):
                at = pl.ds(pl.multiple_of(t * up_tile, up_tile), up_tile)
                block = rows[pl.ds(base, block_rows), :]
                gate = jnp.dot(block, gate_all[:, at], preferred_element_type=jnp.float32)
                up = jnp.dot(block, up_all[:, at], preferred_element_type=jnp.float32)
                active[:, at] = (jax.nn.silu(gate) * up).astype(jnp.bfloat16)
                return carry

            lax.fori_loop(0, hidden // up_tile, step, 0)

        def leave(s):
            base = s * block_rows
            if not state["left"]:
                loads[2].wait()
                gathers[2].wait_recv()
            state["left"] = True

            def step(t, carry):
                at = pl.ds(pl.multiple_of(t * WIDE, WIDE), WIDE)
                value = jnp.dot(active[...], down_all[:, at], preferred_element_type=jnp.float32)
                partial[pl.ds(base, block_rows), at] = value.astype(jnp.bfloat16)
                return carry

            lax.fori_loop(0, width // WIDE, step, 0)

        def swap(s, side):
            span = pl.ds(side * cap, cap)
            launch(
                remote(
                    partial.at[pl.ds(s * block_rows + (2 + side) * cap, cap)],
                    mirrored.at[s, span],
                    spot(role, False, True),
                    swap_send.at[s, side],
                    swap_recv.at[s, side],
                )
            )

        def finish(s, side):
            arrived = mirrored.at[s, pl.ds(side * cap, cap)]
            expect(arrived, swap_recv.at[s, side]).wait_recv()
            seen = role if s < 2 else last - role
            span = pl.ds(s * block_rows + side * cap, cap)
            total = partial[span].astype(jnp.float32) + arrived[...].astype(jnp.float32)
            if s == role and side == 0:
                back[2 * s] = total.astype(jnp.bfloat16)
                return
            partial[span] = total.astype(jnp.bfloat16)
            launch(
                remote(
                    partial.at[span],
                    back.at[2 * seen + side],
                    spot(s, side == 1, False),
                    back_send.at[2 * s + side],
                    back_recv.at[2 * seen + side],
                )
            )

        def gather(s):
            fresh = not state["summed"]
            state["summed"] = True
            for side in range(2):
                if s != role or side == 1:
                    expect(back.at[2 * s + side], back_recv.at[2 * s + side]).wait_recv()
            for low in range(0, width, WIDE):
                block = back[2 * s : 2 * s + 2, :, low : low + WIDE].reshape(2 * cap, WIDE)
                value = jnp.dot(weigh[s, 0], block, preferred_element_type=jnp.float32)
                value = value + jnp.dot(weigh[s, 1], block, preferred_element_type=jnp.float32)
                held = mixed[:, low : low + WIDE]
                mixed[:, low : low + WIDE] = value if fresh else held + value

        near = spot(1 - role, False, False)
        if role == 0:
            select(0)
            raw_in(4, 0)
            raw_in(4, 1)
            raw_in(1, 1)
            raw_out(2, 4, 4, near, 0)
            raw_in(1, 0)
            select(1)
            x_out(1, 0)
            raw_in(2, 0)
            y_in(0)
            select(4)
            raw_out(2, 4, 4, near, 1)
            y_in(1)
            x_out(1, 1)
            raw_in(2, 1)
            select(2)
            x_out(2, 0)
            y_in(4)
            enter(0)
            leave(0)
            y_in(2)
            x_out(2, 1)
            swap(0, 1)
            x_in(1, 1)
            x_in(1, 0)
            enter(1)
            leave(1)
            raw_in(3, 0)
            raw_in(3, 1)
            select(3)
            x_in(2, 1)
            swap(1, 1)
            x_in(2, 0)
            enter(2)
            leave(2)
            swap(2, 0)
            finish(1, 1)
            raw_in(5, 1)
            raw_in(5, 0)
            select(5)
            swap(2, 1)
            y_in(3)
            finish(2, 0)
            swap(1, 0)
            finish(2, 1)
            swap(0, 0)
            y_in(5)
            enter(3)
            leave(3)
            swap(3, 0)
            finish(0, 1)
            swap(3, 1)
            gather(1)
            finish(1, 0)
            finish(3, 0)
            finish(3, 1)
            finish(0, 0)
            gather(2)
            gather(0)
            gather(3)
        else:
            far = spot(2, False, False)
            select(1)
            x_out(1, 0)
            raw_in(2, 0)
            y_in(1)
            raw_out(3, 2, 2, near, 0)
            x_out(1, 1)
            raw_in(0, 0)
            raw_in(0, 1)
            raw_in(2, 1)
            raw_out(2, 0, 3, far, 0)
            raw_out(3, 2, 2, near, 1)
            select(2)
            x_out(2, 0)
            raw_out(2, 0, 3, far, 1)
            x_in(1, 0)
            select(0)
            x_in(1, 1)
            y_in(2)
            x_out(2, 1)
            raw_in(4, 0)
            raw_out(5, 4, 5, far, 0)
            enter(1)
            leave(1)
            raw_in(3, 0)
            raw_in(3, 1)
            raw_in(4, 1)
            raw_out(4, 3, 3, near, 1)
            raw_out(5, 4, 5, far, 1)
            y_in(0)
            select(4)
            raw_out(4, 3, 3, near, 0)
            swap(1, 0)
            x_in(2, 0)
            x_in(2, 1)
            enter(2)
            leave(2)
            raw_in(5, 0)
            swap(2, 0)
            raw_in(5, 1)
            finish(1, 0)
            select(3)
            swap(2, 1)
            y_in(4)
            select(5)
            raw_out(6, 5, 5, near, 0)
            enter(0)
            leave(0)
            swap(0, 1)
            finish(2, 0)
            swap(0, 0)
            y_in(3)
            raw_out(6, 5, 5, near, 1)
            finish(2, 1)
            y_in(5)
            enter(3)
            leave(3)
            finish(0, 1)
            swap(3, 1)
            swap(3, 0)
            finish(0, 0)
            swap(1, 1)
            gather(2)
            finish(3, 1)
            finish(3, 0)
            finish(1, 1)
            gather(1)
            gather(3)
            gather(0)
        result[...] = (
            middle[...].astype(jnp.float32) + rms_scale(mixed[...], post_ffn_gain[...])
        ).astype(jnp.bfloat16)
        for copy in sent + gathers + [exchange]:
            copy.wait_send()

    for role in range(2):

        @pl.when(own == role)
        def _(role=role):
            program(role)

    @pl.when(place < places - 1)
    def _():
        edge.wait_send()


def body(
    residual,
    projected,
    group_weight,
    channel_scale,
    out_weight,
    post_mix_gain,
    pre_ffn_gain,
    post_ffn_gain,
    route_ids,
    route_weight,
    expert_gate,
    expert_up,
    expert_down,
):
    share, width = residual.shape
    tokens, cut = projected.shape
    experts = lax.axis_size("sp") // 2
    cap = 2 * TOP * share // experts
    quarter = expert_gate.shape[2]
    kinds = jnp.bfloat16
    dma = pltpu.SemaphoreType.DMA
    vmem = pl.BlockSpec(memory_space=pltpu.VMEM)
    hbm = pl.BlockSpec(memory_space=pltpu.HBM)
    if 4 * 4 == lax.axis_size("sp"):
        sizes = [
            (width, 2 * quarter),
            (width, 2 * quarter),
            (2 * quarter, width),
            out_weight.shape,
            (6, share, width),
            (2 * experts * cap, width),
            (6, cap, width),
            (4 * cap, 2 * quarter),
            (2 * experts * cap, width),
            (4, 2 * cap, width),
            (experts, cap, width),
            (2**GROUPS, cut),
            (tokens, cut),
            (share, cut),
        ]
        return pl.pallas_call(
            functools.partial(line_kernel, experts, cap),
            out_shape=jax.ShapeDtypeStruct((share, width), kinds),
            in_specs=[vmem] * 4 + [hbm] + [vmem] * 5 + [hbm] * 3,
            out_specs=vmem,
            scratch_shapes=[pltpu.VMEM(size, kinds) for size in sizes]
            + [
                pltpu.VMEM((share, width), jnp.float32),
                pltpu.VMEM((share, width), kinds),
                pltpu.VMEM((6, 8, share), jnp.int32),
                pltpu.VMEM((6, 2 * cap, share), kinds),
                pltpu.VMEM((4, 2, share, 2 * cap), kinds),
                dma((4,)),
                dma((3,)),
                dma((3,)),
                dma((2,)),
                dma((2,)),
                dma((7,)),
                dma((6,)),
                dma((7, 2)),
                dma((6, 2)),
                dma((6,)),
                dma((6,)),
                dma((4,)),
                dma((4,)),
                dma((4, 2)),
                dma((4, 2)),
                dma((8,)),
                dma((8,)),
            ],
            compiler_params=pltpu.CompilerParams(
                collective_id=0, has_side_effects=True, vmem_limit_bytes=62 * 1024 * 1024
            ),
        )(
            residual,
            projected,
            group_weight,
            channel_scale.reshape(1, cut),
            out_weight,
            post_mix_gain.reshape(1, width),
            pre_ffn_gain.reshape(1, width),
            post_ffn_gain.reshape(1, width),
            route_ids.T,
            route_weight.T,
            expert_gate,
            expert_up,
            expert_down,
        )
    return pl.pallas_call(
        functools.partial(layer_kernel, experts, cap),
        out_shape=jax.ShapeDtypeStruct((share, width), kinds),
        in_specs=[vmem] * 4 + [hbm] + [vmem] * 5 + [hbm] * 3,
        out_specs=vmem,
        scratch_shapes=[
            pltpu.VMEM((width, 2 * quarter), kinds),
            pltpu.VMEM((width, 2 * quarter), kinds),
            pltpu.VMEM((2 * quarter, width), kinds),
            pltpu.VMEM((2 * experts * cap, width), kinds),
            pltpu.VMEM((GROUP_ROWS, 2 * quarter), kinds),
            pltpu.VMEM((2 * experts * cap, width), kinds),
            pltpu.VMEM((experts, cap, width), kinds),
            pltpu.VMEM((experts, cap, width), kinds),
            pltpu.VMEM((experts, cap, width), kinds),
            pltpu.VMEM(out_weight.shape, kinds),
            pltpu.VMEM((2**GROUPS, cut), kinds),
            pltpu.VMEM((tokens, cut), kinds),
            pltpu.VMEM((share, cut), kinds),
            pltpu.VMEM((share, width), jnp.float32),
            pltpu.VMEM((share, width), kinds),
            dma((4,)),
            dma((3,)),
            dma((3,)),
        ]
        + [dma((experts,))] * 8
        + [dma((2,))] * 2,
        compiler_params=pltpu.CompilerParams(
            collective_id=0, has_side_effects=True, vmem_limit_bytes=62 * 1024 * 1024
        ),
    )(
        residual,
        projected,
        group_weight,
        channel_scale.reshape(1, cut),
        out_weight,
        post_mix_gain.reshape(1, width),
        pre_ffn_gain.reshape(1, width),
        post_ffn_gain.reshape(1, width),
        route_ids,
        route_weight,
        expert_gate,
        expert_up,
        expert_down,
    )


def solution(mesh):
    in_specs = (
        P(("sp", "tp"), None),
        P("sp", "tp"),
        P("tp", None, None),
        P("tp"),
        P(),
        P(),
        P(),
        P(),
        P(("sp", "tp"), None),
        P(("sp", "tp"), None),
        P("sp", None, "tp"),
        P("sp", None, "tp"),
        P("sp", "tp", None),
    )
    out_specs = P(("sp", "tp"), None)
    return jax.shard_map(body, mesh=mesh, in_specs=in_specs, out_specs=out_specs, check_vma=False)
```

```python
import functools

import jax
import jax.numpy as jnp
from jax import lax
from jax.experimental import pallas as pl
from jax.experimental.pallas import tpu as pltpu
from jax.sharding import PartitionSpec as P

GROUPS = 4
TOP = 2


EPS = 1e-06
MESH = pl.DeviceIdType.MESH
TILE = 256
WIDE = 512
GROUP_ROWS = 256


def rms_scale(values, gain):
    inverse = lax.rsqrt(jnp.mean(values * values, axis=-1, keepdims=True) + EPS)
    return values * inverse * gain


def flipped(index, mask, count):
    result = 0
    bit = 1
    while bit < count:
        digit = (index // bit) % 2
        result = result + (1 - digit if mask & bit else digit) * bit
        bit = bit * 2
    return result


def layer_kernel(
    experts,
    cap,
    residual,
    projected,
    group_weight,
    channel_scale,
    out_hbm,
    post_mix_gain,
    pre_ffn_gain,
    post_ffn_gain,
    route_ids,
    route_weight,
    gate_hbm,
    up_hbm,
    down_hbm,
    result,
    gate_all,
    up_all,
    down_all,
    rows,
    active,
    partial,
    mirrored,
    table,
    back,
    out_all,
    halo,
    scaled,
    received,
    mixed,
    middle,
    local_sem,
    weight_send,
    weight_recv,
    out_send,
    out_recv,
    twin_send,
    twin_recv,
    swap_send,
    swap_recv,
    back_send,
    back_recv,
    front_send,
    front_recv,
):
    place = lax.axis_index("sp")
    core = lax.axis_index("tp")
    expert, side = place // 2, place % 2
    twin = (place + 1 - 2 * side, core)
    partner = (place, 1 - core)
    peers = [None] + [(2 * flipped(expert, r, experts) + side, core) for r in range(1, experts)]
    quarter = gate_hbm.shape[2]
    hidden = 2 * quarter
    width = residual.shape[1]
    half_rows = GROUP_ROWS // 2
    per_group = half_rows // cap
    places = lax.axis_size("sp")
    tokens = projected.shape[0]
    share = tokens // 2
    cut = projected.shape[1]
    lookback = halo.shape[0]
    groups = experts // per_group

    def spot(r, mirror):
        return (r // per_group) * GROUP_ROWS + mirror * half_rows + (r % per_group) * cap

    def send(source, target, device, first, second):
        copy = pltpu.make_async_remote_copy(
            src_ref=source,
            dst_ref=target,
            send_sem=first,
            recv_sem=second,
            device_id=device,
            device_id_type=MESH,
        )
        copy.start()
        return copy

    weights = [
        (gate_hbm.at[0], gate_all.at[:, pl.ds(0, quarter)], gate_all.at[:, pl.ds(quarter, quarter)]),
        (up_hbm.at[0], up_all.at[:, pl.ds(0, quarter)], up_all.at[:, pl.ds(quarter, quarter)]),
        (down_hbm.at[0], down_all.at[pl.ds(0, quarter)], down_all.at[pl.ds(quarter, quarter)]),
    ]
    out_load = pltpu.make_async_copy(out_hbm, out_all, local_sem.at[3])
    out_load.start()
    loads = []
    for i, (source, own, _) in enumerate(weights):
        load = pltpu.make_async_copy(source, own, local_sem.at[i])
        load.start()
        loads.append(load)

    barrier = pltpu.get_barrier_semaphore()
    ring = [((place + 1) % places, core), ((place + places - 1) % places, core)]
    for device in peers[1:] + [twin, partner] + ring:
        pl.semaphore_signal(barrier, inc=1, device_id=device, device_id_type=MESH)
    pl.semaphore_wait(barrier, experts + 3)

    edge = pltpu.make_async_remote_copy(
        src_ref=projected.at[pl.ds(tokens - lookback, lookback)],
        dst_ref=halo,
        send_sem=front_send.at[0],
        recv_sem=front_recv.at[0],
        device_id=ring[0],
        device_id_type=MESH,
    )

    @pl.when(place < places - 1)
    def _():
        edge.start()

    columns = lax.broadcasted_iota(jnp.int32, (share, experts * cap), 1)
    owner = (columns // cap) ^ expert
    named = [owner == route_ids[:, k : k + 1] for k in range(TOP)]
    member = functools.reduce(jnp.logical_or, named).astype(jnp.float32)
    earlier = (
        lax.broadcasted_iota(jnp.int32, (share, share), 1)
        < lax.broadcasted_iota(jnp.int32, (share, share), 0)
    ).astype(jnp.bfloat16)
    rank = jnp.dot(earlier, member.astype(jnp.bfloat16), preferred_element_type=jnp.float32)
    chosen = jnp.where(rank == (columns % cap).astype(jnp.float32), member, 0.0)
    spread = chosen.T.astype(jnp.bfloat16)
    picks = [jnp.where(hit, chosen, 0.0).astype(jnp.bfloat16) for hit in named]

    @pl.when(place > 0)
    def _():
        edge.wait_recv()

    @pl.when(place == 0)
    def _():
        halo[...] = jnp.zeros_like(halo)

    position = (
        place * tokens + lax.broadcasted_iota(jnp.int32, (tokens, 1), 0) + 1
    ).astype(jnp.float32)
    groups_here = group_weight.shape[0]
    group_width = cut // groups_here
    for local_group in range(groups_here):
        low = local_group * group_width
        own_part = projected[:, low : low + group_width].astype(jnp.float32)
        current = jnp.concatenate(
            [halo[:, low : low + group_width].astype(jnp.float32), own_part], 0
        )
        group_id = core * groups_here + local_group
        summed = own_part
        window_span = jnp.float32(1.0)
        for level_id in range(GROUPS):
            current = current + pltpu.roll(current, 2**level_id, 0)
            hit = group_id == level_id
            summed = jnp.where(hit, current[lookback:], summed)
            window_span = jnp.where(hit, jnp.float32(2.0 ** (level_id + 1)), window_span)
        pooled = (summed / jnp.minimum(position, window_span) - own_part).astype(jnp.bfloat16)
        grouped = jnp.dot(pooled, group_weight[local_group], preferred_element_type=jnp.float32)
        scaled[:, low : low + group_width] = (
            grouped * channel_scale[:, low : low + group_width]
        ).astype(jnp.bfloat16)
    there = pl.ds(pl.multiple_of((1 - core) * share, share), share)
    here = pl.ds(pl.multiple_of(core * share, share), share)
    exchange = send(scaled.at[there], received, partner, front_send.at[1], front_recv.at[1])
    out_load.wait()

    def mix(block, first_row, fresh):
        def step(t, carry):
            at = pl.ds(pl.multiple_of(t * WIDE, WIDE), WIDE)
            value = jnp.dot(
                block, out_all[pl.ds(first_row, cut), at], preferred_element_type=jnp.float32
            )
            mixed[:, at] = value if fresh else mixed[:, at] + value
            return carry

        lax.fori_loop(0, width // WIDE, step, 0)

    mix(scaled[here], pl.multiple_of(core * cut, cut), True)
    exchange.wait_recv()
    gathers = [
        send(source, theirs, partner, weight_send.at[i], weight_recv.at[i])
        for i, (source, _, theirs) in enumerate(weights)
    ]
    mix(received[...], pl.multiple_of((1 - core) * cut, cut), False)
    rounded = mixed[...].astype(jnp.bfloat16).astype(jnp.float32)
    kept = residual[...].astype(jnp.float32) + rms_scale(rounded, post_mix_gain[...])
    middle[...] = kept.astype(jnp.bfloat16)
    normed = rms_scale(middle[...].astype(jnp.float32), pre_ffn_gain[...]).astype(jnp.bfloat16)
    for low in range(0, width, WIDE):
        block = jnp.dot(spread, normed[:, low : low + WIDE], preferred_element_type=jnp.float32)
        table[:, :, low : low + WIDE] = block.astype(jnp.bfloat16).reshape(experts, cap, WIDE)
    rows[pl.ds(spot(0, 0), cap)] = table[0]

    outs = [None] + [
        send(
            table.at[r],
            rows.at[pl.ds(spot(r, 0), cap)],
            peers[r],
            out_send.at[r],
            out_recv.at[r],
        )
        for r in range(1, experts)
    ]
    twins = [None] * experts
    twins[0] = send(
        table.at[0], rows.at[pl.ds(spot(0, 1), cap)], twin, twin_send.at[0], twin_recv.at[0]
    )
    swaps = [None] * experts
    backs = [None] * experts

    def forward(g):
        for r in range(g * per_group, (g + 1) * per_group):
            if r > 0:
                outs[r].wait_recv()
                twins[r] = send(
                    rows.at[pl.ds(spot(r, 0), cap)],
                    rows.at[pl.ds(spot(r, 1), cap)],
                    twin,
                    twin_send.at[r],
                    twin_recv.at[r],
                )

    def compute(g):
        base = g * GROUP_ROWS
        for r in range(g * per_group, (g + 1) * per_group):
            twins[r].wait_recv()
        if g == 0:
            for i in range(2):
                loads[i].wait()
                gathers[i].wait_recv()

        def enter(t, carry):
            at = pl.ds(pl.multiple_of(t * TILE, TILE), TILE)
            here = rows[pl.ds(base, GROUP_ROWS), :]
            gate = jnp.dot(here, gate_all[:, at], preferred_element_type=jnp.float32)
            up = jnp.dot(here, up_all[:, at], preferred_element_type=jnp.float32)
            active[:, at] = (jax.nn.silu(gate) * up).astype(jnp.bfloat16)
            return carry

        lax.fori_loop(0, hidden // TILE, enter, 0)
        if g == 0:
            loads[2].wait()
            gathers[2].wait_recv()

        def leave(t, carry):
            at = pl.ds(pl.multiple_of(t * TILE, TILE), TILE)
            value = jnp.dot(active[...], down_all[:, at], preferred_element_type=jnp.float32)
            partial[pl.ds(base, GROUP_ROWS), at] = value.astype(jnp.bfloat16)
            return carry

        lax.fori_loop(0, width // TILE, leave, 0)

    def swap(g):
        for r in range(g * per_group, (g + 1) * per_group):
            swaps[r] = send(
                partial.at[pl.ds(spot(r, 1), cap)],
                mirrored.at[r],
                twin,
                swap_send.at[r],
                swap_recv.at[r],
            )

    def finish(g):
        for r in range(g * per_group, (g + 1) * per_group):
            piece = pl.ds(spot(r, 0), cap)
            swaps[r].wait_recv()
            total = partial[piece].astype(jnp.float32) + mirrored[r].astype(jnp.float32)
            partial[piece] = total.astype(jnp.bfloat16)
            if r > 0:
                backs[r] = send(
                    partial.at[piece], back.at[r], peers[r], back_send.at[r], back_recv.at[r]
                )
            else:
                back[0] = partial[piece]

    forward(0)
    forward(1)
    compute(0)
    forward(2)
    swap(0)
    compute(2)
    swap(2)
    forward(3)
    compute(1)
    swap(1)
    finish(0)
    finish(2)
    compute(3)
    swap(3)
    finish(1)
    finish(3)
    for r in range(1, experts):
        backs[r].wait_recv()
    flat = back[...].reshape(experts * cap, width)
    for low in range(0, width, WIDE):
        total = jnp.zeros((share, WIDE), jnp.float32)
        for k in range(TOP):
            picked = jnp.dot(
                picks[k], flat[:, low : low + WIDE], preferred_element_type=jnp.float32
            )
            total = total + picked * route_weight[:, k : k + 1]
        mixed[:, low : low + WIDE] = total
    result[...] = (
        middle[...].astype(jnp.float32) + rms_scale(mixed[...], post_ffn_gain[...])
    ).astype(jnp.bfloat16)
    for r in range(1, experts):
        backs[r].wait_send()
        outs[r].wait_send()
    for copy in twins + swaps + gathers + [exchange]:
        copy.wait_send()

    @pl.when(place < places - 1)
    def _():
        edge.wait_send()


def line_kernel(
    experts,
    cap,
    residual,
    projected,
    group_weight,
    channel_scale,
    out_hbm,
    post_mix_gain,
    pre_ffn_gain,
    post_ffn_gain,
    route_ids,
    route_weight,
    gate_hbm,
    up_hbm,
    down_hbm,
    result,
    gate_all,
    up_all,
    down_all,
    out_all,
    raw,
    rows,
    across,
    active,
    partial,
    mirrored,
    back,
    halo,
    scaled,
    received,
    mixed,
    middle,
    ids,
    picks,
    weigh,
    local_sem,
    weight_send,
    weight_recv,
    front_send,
    front_recv,
    ids_send,
    ids_recv,
    raw_send,
    raw_recv,
    y_send,
    y_recv,
    x_send,
    x_recv,
    swap_send,
    swap_recv,
    back_send,
    back_recv,
):
    place = lax.axis_index("sp")
    core = lax.axis_index("tp")
    places = lax.axis_size("sp")
    planes = places // 4
    last = planes - 1
    z, y, x = place // 4, (place // 2) % 2, place % 2
    half = z // (planes // 2)
    inward = 1 - 2 * half
    own = (z + half) % 2
    partner = (place, 1 - core)
    quarter = gate_hbm.shape[2]
    hidden = 2 * quarter
    share, width = residual.shape
    tokens, cut = projected.shape
    lookback = halo.shape[0]
    block_rows = 4 * cap
    piece = share // 2
    finer = cap // 2
    up_tile = hidden // 2

    def spot(s, other_y, other_x):
        at_z = s + half * (last - 2 * s)
        at_y = 1 - y if other_y else y
        at_x = 1 - x if other_x else x
        return (at_z * 4 + at_y * 2 + at_x, core)

    def remote(source, target, device, first, second):
        return pltpu.make_async_remote_copy(
            src_ref=source,
            dst_ref=target,
            send_sem=first,
            recv_sem=second,
            device_id=device,
            device_id_type=MESH,
        )

    weights = [
        (gate_hbm.at[0], gate_all.at[:, pl.ds(0, quarter)], gate_all.at[:, pl.ds(quarter, quarter)]),
        (up_hbm.at[0], up_all.at[:, pl.ds(0, quarter)], up_all.at[:, pl.ds(quarter, quarter)]),
        (down_hbm.at[0], down_all.at[pl.ds(0, quarter)], down_all.at[pl.ds(quarter, quarter)]),
    ]
    out_load = pltpu.make_async_copy(out_hbm, out_all, local_sem.at[3])
    out_load.start()
    loads = []
    for i, (source, mine, _) in enumerate(weights):
        load = pltpu.make_async_copy(source, mine, local_sem.at[i])
        load.start()
        loads.append(load)

    barrier = pltpu.get_barrier_semaphore()
    for step in range(1, places):
        device = ((place + step) % places, core)
        pl.semaphore_signal(barrier, inc=1, device_id=device, device_id_type=MESH)
    pl.semaphore_signal(barrier, inc=1, device_id=partner, device_id_type=MESH)
    pl.semaphore_wait(barrier, places)

    edge = remote(
        projected.at[pl.ds(tokens - lookback, lookback)],
        halo,
        ((place + 1) % places, core),
        front_send.at[0],
        front_recv.at[0],
    )

    @pl.when(place < places - 1)
    def _():
        edge.start()

    ids[own] = jnp.concatenate(
        [route_ids[...], jnp.zeros((ids.shape[1] - TOP, share), jnp.int32)], 0
    )

    def id_copies(role):
        if role == 0:
            targets = [(1, False, 0), (2, False, 3), (3, False, 3)]
            targets += [(0, True, 4), (1, True, 4), (2, True, 5), (3, True, 5)]
        else:
            targets = [(0, False, 1), (2, False, 2), (3, False, 2)]
        return [
            remote(ids.at[role], ids.at[j], spot(s, False, turn), ids_send.at[i], ids_recv.at[j])
            for i, (s, turn, j) in enumerate(targets)
        ]

    def expect(target, semaphore):
        return remote(target, target, partner, local_sem.at[0], semaphore)

    for role in range(2):

        @pl.when(own == role)
        def _(role=role):
            for copy in id_copies(role):
                copy.start()

    @pl.when(place > 0)
    def _():
        edge.wait_recv()

    @pl.when(place == 0)
    def _():
        halo[...] = jnp.zeros_like(halo)

    position = (
        place * tokens + lax.broadcasted_iota(jnp.int32, (tokens, 1), 0) + 1
    ).astype(jnp.float32)
    groups_here = group_weight.shape[0]
    group_width = cut // groups_here
    for local_group in range(groups_here):
        low = local_group * group_width
        own_part = projected[:, low : low + group_width].astype(jnp.float32)
        current = jnp.concatenate(
            [halo[:, low : low + group_width].astype(jnp.float32), own_part], 0
        )
        group_id = core * groups_here + local_group
        summed = own_part
        window_span = jnp.float32(1.0)
        for level_id in range(GROUPS):
            current = current + pltpu.roll(current, 2**level_id, 0)
            hit = group_id == level_id
            summed = jnp.where(hit, current[lookback:], summed)
            window_span = jnp.where(hit, jnp.float32(2.0 ** (level_id + 1)), window_span)
        pooled = (summed / jnp.minimum(position, window_span) - own_part).astype(jnp.bfloat16)
        grouped = jnp.dot(pooled, group_weight[local_group], preferred_element_type=jnp.float32)
        scaled[:, low : low + group_width] = (
            grouped * channel_scale[:, low : low + group_width]
        ).astype(jnp.bfloat16)
    there = pl.ds(pl.multiple_of((1 - core) * share, share), share)
    here = pl.ds(pl.multiple_of(core * share, share), share)
    exchange = remote(scaled.at[there], received, partner, front_send.at[1], front_recv.at[1])
    exchange.start()
    out_load.wait()

    def mix(block, first_row, fresh):
        def step(t, carry):
            at = pl.ds(pl.multiple_of(t * WIDE, WIDE), WIDE)
            value = jnp.dot(
                block, out_all[pl.ds(first_row, cut), at], preferred_element_type=jnp.float32
            )
            mixed[:, at] = value if fresh else mixed[:, at] + value
            return carry

        lax.fori_loop(0, width // WIDE, step, 0)

    mix(scaled[here], pl.multiple_of(core * cut, cut), True)
    exchange.wait_recv()
    gathers = [
        remote(source, theirs, partner, weight_send.at[i], weight_recv.at[i])
        for i, (source, _, theirs) in enumerate(weights)
    ]
    for copy in gathers:
        copy.start()
    mix(received[...], pl.multiple_of((1 - core) * cut, cut), False)
    rounded = mixed[...].astype(jnp.bfloat16).astype(jnp.float32)
    kept = residual[...].astype(jnp.float32) + rms_scale(rounded, post_mix_gain[...])
    middle[...] = kept.astype(jnp.bfloat16)
    raw[own] = rms_scale(middle[...].astype(jnp.float32), pre_ffn_gain[...]).astype(jnp.bfloat16)

    def raw_copy(number, source, target, device, part):
        span = pl.ds(part * piece, piece)
        return remote(
            raw.at[source, span],
            raw.at[target, span],
            device,
            raw_send.at[number, part],
            raw_recv.at[target, part],
        )

    def first_copies(role):
        near, twin = spot(1 - role, False, False), spot(role, False, True)
        copies = []
        for part in range(2):
            if role == 0:
                copies.append(raw_copy(0, 0, 0, near, part))
                copies.append(raw_copy(1, 0, 4, twin, part))
            else:
                copies.append(raw_copy(0, 1, 1, near, part))
                copies.append(raw_copy(1, 1, 2, spot(2, False, False), part))
        return copies

    for role in range(2):

        @pl.when(own == role)
        def _(role=role):
            for copy in first_copies(role):
                copy.start()

    for role in range(2):

        @pl.when(own == role)
        def _(role=role):
            for j in range(6):
                if j != role:
                    expect(ids.at[j], ids_recv.at[j]).wait_recv()

    sub = lax.broadcasted_iota(jnp.int32, (8, share), 0)
    here_expert = 2 * z + jnp.where(sub == 0, y, 1 - y)
    at = sub // 2
    turn = sub % 2
    home_expert = 2 * (at + half * (last - 2 * at)) + (y + turn - 2 * y * turn)
    members = []
    for j in range(6):
        first, second = ids[j, 0:1, :], ids[j, 1:2, :]
        named = jnp.logical_or(first == here_expert, second == here_expert)
        members.append(jnp.where(jnp.logical_and(named, sub < 2), 1.0, 0.0))
    first, second = route_ids[0:1, :] == home_expert, route_ids[1:2, :] == home_expert
    members.append(jnp.where(jnp.logical_or(first, second), 1.0, 0.0))
    factor = jnp.where(first, route_weight[0:1, :], 0.0) + jnp.where(
        second, route_weight[1:2, :], 0.0
    )
    member = jnp.concatenate(members, 0)
    earlier = jnp.where(
        lax.broadcasted_iota(jnp.int32, (share, share), 0)
        < lax.broadcasted_iota(jnp.int32, (share, share), 1),
        1.0,
        0.0,
    ).astype(jnp.bfloat16)
    rank = jnp.dot(member.astype(jnp.bfloat16), earlier, preferred_element_type=jnp.float32)
    slot = lax.broadcasted_iota(jnp.int32, (cap, share), 0).astype(jnp.float32)
    for j in range(6):
        pair = [
            jnp.where(rank[8 * j + i : 8 * j + i + 1] == slot, member[8 * j + i : 8 * j + i + 1], 0.0)
            for i in range(2)
        ]
        picks[j] = jnp.concatenate(pair, 0).astype(jnp.bfloat16)
    for s in range(4):
        pair = [
            jnp.where(rank[48 + i : 49 + i] == slot, factor[i : i + 1], 0.0)
            for i in (2 * s, 2 * s + 1)
        ]
        full = jnp.concatenate(pair, 0).T
        high = full.astype(jnp.bfloat16)
        weigh[s, 0] = high
        weigh[s, 1] = (full - high.astype(jnp.float32)).astype(jnp.bfloat16)

    def program(role):
        sent = id_copies(role) + first_copies(role)
        state = {"entered": False, "left": False, "summed": False}

        def launch(copy):
            copy.start()
            sent.append(copy)

        def raw_out(*hop):
            launch(raw_copy(*hop))

        def raw_in(j, part):
            span = pl.ds(part * piece, piece)
            expect(raw.at[j, span], raw_recv.at[j, part]).wait_recv()

        def row_of(j):
            return j * block_rows if j < 4 else (j - 4) * 3 * block_rows + 2 * cap

        def select(j):
            low = row_of(j)

            def step(t, carry):
                at = pl.ds(pl.multiple_of(t * WIDE, WIDE), WIDE)
                value = jnp.dot(picks[j], raw[j, :, at], preferred_element_type=jnp.float32)
                value = value.astype(jnp.bfloat16)
                rows[pl.ds(low, cap), at] = value[:cap]
                across[j, :, at] = value[cap:]
                return carry

            lax.fori_loop(0, width // WIDE, step, 0)
            launch(
                remote(
                    across.at[j],
                    rows.at[pl.ds(low + cap, cap)],
                    spot(role, True, False),
                    y_send.at[j],
                    y_recv.at[j],
                )
            )

        def y_in(j):
            expect(rows.at[pl.ds(row_of(j) + cap, cap)], y_recv.at[j]).wait_recv()

        def x_out(s, side):
            low = s * block_rows + side * cap
            number = 2 * (s - 1) + side
            launch(
                remote(
                    rows.at[pl.ds(low, cap)],
                    rows.at[pl.ds(low + 2 * cap, cap)],
                    spot(role, False, True),
                    x_send.at[number],
                    x_recv.at[number],
                )
            )

        def x_in(s, side):
            low = s * block_rows + (2 + side) * cap
            expect(rows.at[pl.ds(low, cap)], x_recv.at[2 * (s - 1) + side]).wait_recv()

        def enter(s, part=None):
            base = s * block_rows + (part or 0) * 2 * cap
            count = block_rows if part is None else 2 * cap
            if not state["entered"]:
                for i in range(2):
                    loads[i].wait()
                    gathers[i].wait_recv()
            state["entered"] = True

            def step(t, carry):
                at = pl.ds(pl.multiple_of(t * up_tile, up_tile), up_tile)
                block = rows[pl.ds(base, count), :]
                gate = jnp.dot(block, gate_all[:, at], preferred_element_type=jnp.float32)
                up = jnp.dot(block, up_all[:, at], preferred_element_type=jnp.float32)
                active[:count, at] = (jax.nn.silu(gate) * up).astype(jnp.bfloat16)
                return carry

            lax.fori_loop(0, hidden // up_tile, step, 0)

        def leave(s, part=None):
            base = s * block_rows + (part or 0) * 2 * cap
            count = block_rows if part is None else 2 * cap
            if not state["left"]:
                loads[2].wait()
                gathers[2].wait_recv()
            state["left"] = True

            def step(t, carry):
                at = pl.ds(pl.multiple_of(t * WIDE, WIDE), WIDE)
                value = jnp.dot(active[:count, :], down_all[:, at], preferred_element_type=jnp.float32)
                partial[pl.ds(base, count), at] = value.astype(jnp.bfloat16)
                return carry

            lax.fori_loop(0, width // WIDE, step, 0)

        def swap(s, side):
            for part in range(2):
                low = side * cap + part * finer
                launch(
                    remote(
                        partial.at[pl.ds(s * block_rows + 2 * cap + low, finer)],
                        mirrored.at[s, pl.ds(low, finer)],
                        spot(role, False, True),
                        swap_send.at[s, side, part],
                        swap_recv.at[s, side, part],
                    )
                )

        def finish(s, side):
            seen = role if s < 2 else last - role
            for part in range(2):
                low = side * cap + part * finer
                arrived = mirrored.at[s, pl.ds(low, finer)]
                expect(arrived, swap_recv.at[s, side, part]).wait_recv()
                span = pl.ds(s * block_rows + low, finer)
                total = partial[span].astype(jnp.float32) + arrived[...].astype(jnp.float32)
                if s == role and side == 0:
                    back[2 * s, pl.ds(part * finer, finer)] = total.astype(jnp.bfloat16)
                    continue
                partial[span] = total.astype(jnp.bfloat16)
                launch(
                    remote(
                        partial.at[span],
                        back.at[2 * seen + side, pl.ds(part * finer, finer)],
                        spot(s, side == 1, False),
                        back_send.at[2 * s + side, part],
                        back_recv.at[2 * seen + side, part],
                    )
                )

        def gather(s):
            fresh = not state["summed"]
            state["summed"] = True
            for side in range(2):
                if s != role or side == 1:
                    for part in range(2):
                        piece_in = back.at[2 * s + side, pl.ds(part * finer, finer)]
                        expect(piece_in, back_recv.at[2 * s + side, part]).wait_recv()
            for low in range(0, width, WIDE):
                block = back[2 * s : 2 * s + 2, :, low : low + WIDE].reshape(2 * cap, WIDE)
                value = jnp.dot(weigh[s, 0], block, preferred_element_type=jnp.float32)
                value = value + jnp.dot(weigh[s, 1], block, preferred_element_type=jnp.float32)
                held = mixed[:, low : low + WIDE]
                mixed[:, low : low + WIDE] = value if fresh else held + value

        near = spot(1 - role, False, False)
        if role == 0:
            select(0)
            raw_in(4, 0)
            raw_out(2, 4, 4, near, 0)
            raw_in(1, 0)
            raw_in(1, 1)
            select(1)
            x_out(1, 0)
            raw_in(4, 1)
            raw_out(2, 4, 4, near, 1)
            select(4)
            y_in(1)
            x_out(1, 1)
            raw_in(2, 0)
            raw_in(2, 1)
            select(2)
            x_out(2, 0)
            y_in(0)
            y_in(4)
            enter(0)
            y_in(2)
            x_out(2, 1)
            leave(0)
            swap(0, 1)
            x_in(1, 0)
            x_in(1, 1)
            enter(1)
            raw_in(3, 0)
            raw_in(3, 1)
            select(3)
            leave(1)
            swap(1, 1)
            x_in(2, 0)
            x_in(2, 1)
            enter(2)
            raw_in(5, 0)
            raw_in(5, 1)
            select(5)
            leave(2)
            swap(2, 1)
            swap(2, 0)
            y_in(3)
            enter(3, 0)
            leave(3, 0)
            finish(2, 1)
            y_in(5)
            enter(3, 1)
            leave(3, 1)
            swap(3, 1)
            swap(3, 0)
            swap(1, 0)
            swap(0, 0)
            finish(2, 0)
            finish(1, 1)
            finish(0, 1)
            finish(3, 1)
            finish(3, 0)
            finish(1, 0)
            gather(1)
            gather(2)
            finish(0, 0)
            gather(0)
            gather(3)
        else:
            far = spot(2, False, False)
            select(1)
            x_out(1, 0)
            raw_in(0, 0)
            raw_out(2, 0, 3, far, 0)
            raw_in(2, 0)
            raw_out(3, 2, 2, near, 0)
            y_in(1)
            x_out(1, 1)
            raw_in(0, 1)
            raw_out(2, 0, 3, far, 1)
            raw_in(2, 1)
            raw_out(3, 2, 2, near, 1)
            select(2)
            x_out(2, 0)
            select(0)
            x_in(1, 0)
            x_in(1, 1)
            y_in(2)
            x_out(2, 1)
            enter(1)
            raw_in(3, 0)
            raw_out(4, 3, 3, near, 0)
            raw_in(4, 0)
            raw_out(5, 4, 5, far, 0)
            leave(1)
            raw_in(3, 1)
            raw_out(4, 3, 3, near, 1)
            raw_in(4, 1)
            raw_out(5, 4, 5, far, 1)
            swap(1, 0)
            select(4)
            select(3)
            x_in(2, 0)
            x_in(2, 1)
            enter(2)
            raw_in(5, 0)
            raw_out(6, 5, 5, near, 0)
            leave(2)
            swap(2, 0)
            swap(2, 1)
            raw_in(5, 1)
            raw_out(6, 5, 5, near, 1)
            select(5)
            finish(1, 0)
            y_in(0)
            y_in(4)
            enter(0)
            finish(2, 0)
            leave(0)
            swap(0, 1)
            swap(0, 0)
            finish(2, 1)
            y_in(3)
            y_in(5)
            enter(3)
            finish(0, 1)
            leave(3)
            swap(3, 1)
            swap(3, 0)
            swap(1, 1)
            finish(0, 0)
            gather(2)
            finish(3, 1)
            finish(3, 0)
            finish(1, 1)
            gather(3)
            gather(1)
            gather(0)
        result[...] = (
            middle[...].astype(jnp.float32) + rms_scale(mixed[...], post_ffn_gain[...])
        ).astype(jnp.bfloat16)
        for copy in sent + gathers + [exchange]:
            copy.wait_send()

    for role in range(2):

        @pl.when(own == role)
        def _(role=role):
            program(role)

    @pl.when(place < places - 1)
    def _():
        edge.wait_send()


def body(
    residual,
    projected,
    group_weight,
    channel_scale,
    out_weight,
    post_mix_gain,
    pre_ffn_gain,
    post_ffn_gain,
    route_ids,
    route_weight,
    expert_gate,
    expert_up,
    expert_down,
):
    share, width = residual.shape
    tokens, cut = projected.shape
    experts = lax.axis_size("sp") // 2
    cap = 2 * TOP * share // experts
    quarter = expert_gate.shape[2]
    kinds = jnp.bfloat16
    dma = pltpu.SemaphoreType.DMA
    vmem = pl.BlockSpec(memory_space=pltpu.VMEM)
    hbm = pl.BlockSpec(memory_space=pltpu.HBM)
    if 4 * 4 == lax.axis_size("sp"):
        sizes = [
            (width, 2 * quarter),
            (width, 2 * quarter),
            (2 * quarter, width),
            out_weight.shape,
            (6, share, width),
            (2 * experts * cap, width),
            (6, cap, width),
            (4 * cap, 2 * quarter),
            (2 * experts * cap, width),
            (4, 2 * cap, width),
            (experts, cap, width),
            (2**GROUPS, cut),
            (tokens, cut),
            (share, cut),
        ]
        return pl.pallas_call(
            functools.partial(line_kernel, experts, cap),
            out_shape=jax.ShapeDtypeStruct((share, width), kinds),
            in_specs=[vmem] * 4 + [hbm] + [vmem] * 5 + [hbm] * 3,
            out_specs=vmem,
            scratch_shapes=[pltpu.VMEM(size, kinds) for size in sizes]
            + [
                pltpu.VMEM((share, width), jnp.float32),
                pltpu.VMEM((share, width), kinds),
                pltpu.VMEM((6, 8, share), jnp.int32),
                pltpu.VMEM((6, 2 * cap, share), kinds),
                pltpu.VMEM((4, 2, share, 2 * cap), kinds),
                dma((4,)),
                dma((3,)),
                dma((3,)),
                dma((2,)),
                dma((2,)),
                dma((7,)),
                dma((6,)),
                dma((7, 2)),
                dma((6, 2)),
                dma((6,)),
                dma((6,)),
                dma((4,)),
                dma((4,)),
                dma((4, 2, 2)),
                dma((4, 2, 2)),
                dma((8, 2)),
                dma((8, 2)),
            ],
            compiler_params=pltpu.CompilerParams(
                collective_id=0, has_side_effects=True, vmem_limit_bytes=62 * 1024 * 1024
            ),
        )(
            residual,
            projected,
            group_weight,
            channel_scale.reshape(1, cut),
            out_weight,
            post_mix_gain.reshape(1, width),
            pre_ffn_gain.reshape(1, width),
            post_ffn_gain.reshape(1, width),
            route_ids.T,
            route_weight.T,
            expert_gate,
            expert_up,
            expert_down,
        )
    return pl.pallas_call(
        functools.partial(layer_kernel, experts, cap),
        out_shape=jax.ShapeDtypeStruct((share, width), kinds),
        in_specs=[vmem] * 4 + [hbm] + [vmem] * 5 + [hbm] * 3,
        out_specs=vmem,
        scratch_shapes=[
            pltpu.VMEM((width, 2 * quarter), kinds),
            pltpu.VMEM((width, 2 * quarter), kinds),
            pltpu.VMEM((2 * quarter, width), kinds),
            pltpu.VMEM((2 * experts * cap, width), kinds),
            pltpu.VMEM((GROUP_ROWS, 2 * quarter), kinds),
            pltpu.VMEM((2 * experts * cap, width), kinds),
            pltpu.VMEM((experts, cap, width), kinds),
            pltpu.VMEM((experts, cap, width), kinds),
            pltpu.VMEM((experts, cap, width), kinds),
            pltpu.VMEM(out_weight.shape, kinds),
            pltpu.VMEM((2**GROUPS, cut), kinds),
            pltpu.VMEM((tokens, cut), kinds),
            pltpu.VMEM((share, cut), kinds),
            pltpu.VMEM((share, width), jnp.float32),
            pltpu.VMEM((share, width), kinds),
            dma((4,)),
            dma((3,)),
            dma((3,)),
        ]
        + [dma((experts,))] * 8
        + [dma((2,))] * 2,
        compiler_params=pltpu.CompilerParams(
            collective_id=0, has_side_effects=True, vmem_limit_bytes=62 * 1024 * 1024
        ),
    )(
        residual,
        projected,
        group_weight,
        channel_scale.reshape(1, cut),
        out_weight,
        post_mix_gain.reshape(1, width),
        pre_ffn_gain.reshape(1, width),
        post_ffn_gain.reshape(1, width),
        route_ids,
        route_weight,
        expert_gate,
        expert_up,
        expert_down,
    )


def solution(mesh):
    in_specs = (
        P(("sp", "tp"), None),
        P("sp", "tp"),
        P("tp", None, None),
        P("tp"),
        P(),
        P(),
        P(),
        P(),
        P(("sp", "tp"), None),
        P(("sp", "tp"), None),
        P("sp", None, "tp"),
        P("sp", None, "tp"),
        P("sp", "tp", None),
    )
    out_specs = P(("sp", "tp"), None)
    return jax.shard_map(body, mesh=mesh, in_specs=in_specs, out_specs=out_specs, check_vma=False)
```
